512 devices in a mesh: ep: 32 (over z, x), tp: 16 (over y, core).
Axes of the slice: x: 4, y: 8, z: 8, core: 2. Of those that a mesh axis runs over, the one named last changes fastest.
Arguments:
- mix_rows: bfloat16 [8192, 2048], P('ep'), may hold values from -6 to 6
- mix_gain: bfloat16 [2048], replicated, may hold values from 0.099609375 to 1.8984375
- w_query: bfloat16 [1024, 2048], P('tp'), may hold values from -0.125 to 0.125
- w_key: bfloat16 [1024, 2048], P('tp'), may hold values from -0.125 to 0.125
- w_value: bfloat16 [1024, 2048], P('tp'), may hold values from -0.125 to 0.125
- key_offset: float32 [16, 8192], P('tp'), may hold values from -11 to 0
- w_out: bfloat16 [1024, 2048], P('tp'), may hold values from -0.1875 to 0.1875
- out_gain: bfloat16 [2048], replicated, may hold values from 0.099609375 to 1.8984375
- exp_rows: bfloat16 [3072, 2048], P('ep', 'tp'), may hold values from -100 to 100
- exp_gain: bfloat16 [2048], P('tp'), may hold values from 0.099609375 to 1.8984375
- routes: int32 [3072, 4], P('ep'), may hold values from 0 to 31, all different within a row; in each aligned block of 96 rows (0 to 95, 96 to 191, ...) at most 16 rows name the same one
- route_weight: float32 [3072, 4], P('ep'), may hold values from 0.05 to 1
- w_gate: bfloat16 [32, 2048, 2048], P('ep', None, 'tp'), may hold values from -0.5 to 0.5
- w_up: bfloat16 [32, 2048, 2048], P('ep', None, 'tp'), may hold values from -0.5 to 0.5
- w_down: bfloat16 [32, 2048, 2048], P('ep', 'tp'), may hold values from -0.1875 to 0.1875
Outputs:
- mix_out: bfloat16 [8192, 2048], P('ep')
- exp_out: bfloat16 [3072, 2048], P('ep', 'tp')
The draws below stay inside these ranges and needn't reach their ends.
Inputs may be any that keep to these rules, and one draw needn't show every extreme that they name: `routes`: each row names 4 different experts. Within the rows of one device (aligned blocks of 96 rows) no expert is named by more than 16 rows, and in some blocks one expert is named by exactly 16 rows.
All inputs are finite; a program needn't handle non-finite values.
Results may differ from the reference program's by a relative error of at most 0.019.
Values may be sent and summed in bfloat16 or wider, within the bound.
No kernel may reach another device: no remote copies, remote signals or barrier semaphores. Data moves between devices by JAX's collectives and lax.ppermute only.
A program may use at most 128 MiB of HBM per device.

```python
import math
import jax
import jax.numpy as jnp
import numpy as np
from jax import lax

D = 2048
ATTENTION_HEADS = 16
HEAD = 64
FF = 2048
TOPK = 4
MIX_ROWS = 256
EXP_ROWS = 96
EXPERTS = 32
CAP = 16
FF_PART = 128
ATT = 1024
SEQ_LEN = 8192
TOK_B = 3072


def draw_key_offset(key, part):
    starting_key = jax.random.fold_in(key, 101)
    level_key, displacement_key, jitter_key = jax.random.split(starting_key, 3)
    lowest_reach = 0.6
    highest_reach = 1.6
    chain_reach = jax.random.uniform(level_key, (ATTENTION_HEADS, 1), minval=lowest_reach, maxval=highest_reach)
    head_level = jnp.log(chain_reach / SEQ_LEN) - 0.5
    block_shift = jax.random.uniform(displacement_key, (ATTENTION_HEADS, SEQ_LEN // MIX_ROWS), minval=-0.7, maxval=0.7)
    jitter = jax.random.uniform(jitter_key, (ATTENTION_HEADS, SEQ_LEN), minval=-0.5, maxval=0.5)
    offset_values = head_level + jnp.repeat(block_shift, MIX_ROWS, axis=1) + jitter
    return jnp.clip(offset_values, -11.0, 0.0).astype(jnp.float32)


def draw_exp_rows(key, part):
    starting_key = jax.random.fold_in(key, 202)
    noise_key = jax.random.fold_in(starting_key, 0)
    profile = jnp.exp(jnp.linspace(0.0, math.log(6.0), D))[None, :]
    noise = jnp.clip(jax.random.normal(noise_key, (TOK_B, D), jnp.float32), -5.0, 5.0)
    numbers = noise * profile
    return jnp.clip(numbers, -100.0, 100.0).astype(jnp.bfloat16)


def clamp_weights(key, salt):
    starting_key = jax.random.fold_in(key, salt)
    noise_key = jax.random.fold_in(starting_key, 0)
    noise = jnp.clip(jax.random.normal(noise_key, (EXPERTS, D, FF), jnp.float32), -5.0, 5.0) * D ** (-0.5)
    factor = 2.0
    return jnp.clip(noise * factor, -0.5, 0.5).astype(jnp.bfloat16)


def draw_w_gate(key, part):
    return clamp_weights(key, 303)


def draw_w_up(key, part):
    return clamp_weights(key, 404)


def with_spikes(entries, own_key, source, target, shards_of, factor):
    def block_of(position):
        return (jnp.arange(entries.shape[position]) // (entries.shape[position] // shards_of)).reshape((-1,) + (1,) * (entries.ndim - 1 - position))

    first = jax.random.permutation(own_key, shards_of)[block_of(target)]
    other_side = (block_of(target) + shards_of // 2) % shards_of
    return jnp.where((block_of(source) == first) | (block_of(source) == other_side), factor * entries, entries)


def block_scale(rng, extent, cuts, low, high):
    level = 1.0
    for axis_at, shards_of in cuts:
        draws = jax.random.uniform(jax.random.fold_in(jax.random.fold_in(rng, 6), axis_at), (shards_of,), jnp.float32, low / len(cuts), high / len(cuts))
        level = level * jnp.repeat(jnp.exp(draws), extent[axis_at] // shards_of).reshape((-1,) + (1,) * (len(extent) - 1 - axis_at))
    return level


def routed_block(key, own, number, rows, count, top, most, slope):
    ranking = jax.random.permutation(key, count)
    crowded, ordinary = load_shares(count, rows * top, most, slope, True), load_shares(count, rows * top, most, slope, False)
    places = jnp.arange(count)

    def named(sizes, rotation):
        used = int((sizes > 0).sum())
        fixed = max(1, used // 4)
        passed = fixed + (places - fixed + rotation * (used - fixed)) % max(1, count - fixed)
        return jnp.zeros((count,), jnp.int32).at[ranking[jnp.where(places < fixed, places, passed)]].set(jnp.asarray(sizes, jnp.int32))

    sizes = jnp.where(number % 4 == 0, named(crowded, number // 4), named(ordinary, number - number // 4 - 1))
    mixed = jax.random.permutation(jax.random.fold_in(own, 3), count)
    giver, sink = mixed[0:count // 2 * 2:2], mixed[1:count // 2 * 2:2]
    slack = jnp.minimum(sizes[giver] - 1, most - sizes[sink]) // 2
    slack = jnp.where((giver == ranking[0]) | (sink == ranking[0]) | (sizes[sink] == 0), 0, jnp.maximum(slack, 0))
    passed = jax.random.randint(jax.random.fold_in(own, 4), (count // 2,), 0, 1 << 20) % (slack + 1)
    sizes = sizes.at[giver].add(-passed).at[sink].add(passed)
    labels = jnp.searchsorted(jnp.cumsum(sizes), jnp.arange(rows * top), side="right").astype(jnp.int32)
    listing = labels.reshape(top, rows).T
    listing = listing[jax.random.permutation(jax.random.fold_in(own, 1), rows)]
    rotation = jax.random.randint(jax.random.fold_in(own, 2), (rows, 1), 0, top)
    return jnp.take_along_axis(listing, (jnp.arange(top)[None, :] + rotation) % top, axis=1)


def load_shares(amount, total, limit, skew, full):
    portions = [(1 << 20) // math.isqrt(rank ** skew) + 1 for rank in range(1, amount + 1)]
    largest = limit if full else min(limit, max(-(-total // amount), total * portions[0] // sum(portions)))
    least = 1 if total - largest >= amount - 1 else 0
    counts, rest = [largest] + [least] * (amount - 1), total - largest - least * (amount - 1)
    while rest > 0:
        free = [i for i in range(1, amount) if counts[i] < largest] or [i for i in range(1, amount) if counts[i] < limit]
        pool, remaining = sum([portions[i] for i in free]), rest
        for i in free:
            extra = min(limit - counts[i], max(1, remaining * portions[i] // pool), rest)
            counts[i] = counts[i] + extra
            rest = rest - extra
    return np.array(counts)


def bell_draw(own_key, shape, width, reach, shards=(), kind=jnp.bfloat16):
    result = width * jax.random.normal(own_key, shape, jnp.float32)
    if shards:
        result = result * block_scale(own_key, shape, shards, -0.22, 0.18)
    return jnp.clip(result, -reach, reach).astype(kind)


def noise_with(key, extent, spread, reach, cuts, heavy, held_as=jnp.bfloat16):
    array = spread * jax.random.normal(key, extent, jnp.float32)
    if cuts:
        array = array * block_scale(key, extent, cuts, -0.22, 0.18)
    return jnp.clip(with_spikes(array, jax.random.fold_in(key, 3), *heavy), -reach, reach).astype(held_as)


def setup_inputs(seed: int = 0) -> dict:
    arg_keys = jax.random.split(jax.random.key(seed), 16)
    mix_rows = bell_draw(arg_keys[0], (SEQ_LEN, D), 1.0, 6.0, ((0, 32),))
    mix_gain = jnp.clip(1.0 + 0.18 * jax.random.normal(arg_keys[1], (D,), jnp.float32), 0.099609375, 1.8984375).astype(jnp.bfloat16)
    w_query = bell_draw(arg_keys[2], (ATT, D), D ** -0.5, 0.125, ((0, 16),))
    w_key = bell_draw(arg_keys[3], (ATT, D), D ** -0.5, 0.125, ((0, 16),))
    w_value = bell_draw(arg_keys[4], (ATT, D), D ** -0.5, 0.125, ((0, 16),))
    key_offset = draw_key_offset(jax.random.fold_in(arg_keys[15], 71), 0)
    w_out = bell_draw(arg_keys[6], (ATT, D), ATT ** -0.5, 0.1875, ((0, 16),))
    out_gain = jnp.clip(1.0 + 0.18 * jax.random.normal(arg_keys[7], (D,), jnp.float32), 0.099609375, 1.8984375).astype(jnp.bfloat16)
    exp_rows = draw_exp_rows(jax.random.fold_in(arg_keys[15], 71), 0)
    exp_gain = jnp.clip(1.0 + 0.18 * jax.random.normal(arg_keys[9], (D,), jnp.float32), 0.099609375, 1.8984375).astype(jnp.bfloat16)
    routes_keys = jax.random.split(jax.random.fold_in(arg_keys[10], 1), TOK_B // EXP_ROWS)
    routes_turns = jax.random.permutation(jax.random.fold_in(arg_keys[10], 3), TOK_B // EXP_ROWS)
    routes = jax.vmap(lambda own, number: routed_block(jax.random.fold_in(arg_keys[10], 2), own, number, EXP_ROWS, EXPERTS, TOPK, CAP, 1))(routes_keys, routes_turns).reshape((TOK_B, TOPK))
    route_weight = jnp.clip(jnp.exp(math.log(1.0) - 2.9957323 * jax.random.uniform(arg_keys[11], (TOK_B, TOPK), jnp.float32) ** block_scale(arg_keys[11], (TOK_B, TOPK), ((0, 32),), -0.2, 0.2)), 0.05, 1.0)
    w_gate = draw_w_gate(jax.random.fold_in(arg_keys[15], 71), 0)
    w_up = draw_w_up(jax.random.fold_in(arg_keys[15], 71), 0)
    w_down = noise_with(arg_keys[14], (EXPERTS, FF, D), FF ** -0.5, 0.1875, ((0, 32), (1, 16)), (1, 2, 16, 2.0))
    return {"mix_rows": mix_rows, "mix_gain": mix_gain, "w_query": w_query, "w_key": w_key, "w_value": w_value, "key_offset": key_offset, "w_out": w_out, "out_gain": out_gain, "exp_rows": exp_rows, "exp_gain": exp_gain, "routes": routes, "route_weight": route_weight, "w_gate": w_gate, "w_up": w_up, "w_down": w_down}


EPSILON = 1e-06
CLAMP_LIMIT = 7.0
SILU_SHARPNESS = 1.702

def normalize(matrix, gain):
    numbers = matrix.astype(jnp.float32)
    factor = lax.rsqrt(lax.optimization_barrier(jnp.mean(numbers * numbers, axis=-1, keepdims=True)) + EPSILON)
    return numbers * factor * gain.astype(jnp.float32)

def project(normed, weight):
    product = lax.dot_general(normed, weight, (((1,), (1,)), ((), ())), preferred_element_type=jnp.float32)
    return product.astype(jnp.bfloat16)

def stick_weights(scores, visible):
    keep_log = jnp.where(visible, jax.nn.log_sigmoid(-scores), 0.0)
    later_sum = lax.cumsum(keep_log, axis=2, reverse=True) - keep_log
    return jnp.where(visible, jnp.exp(jax.nn.log_sigmoid(scores) + later_sum), 0.0)

def gated_units(gate_pre, up_pre):
    gate_part = jnp.minimum(gate_pre, CLAMP_LIMIT)
    up_part = jnp.clip(up_pre, -CLAMP_LIMIT, CLAMP_LIMIT)
    return (up_part + 1.0) * (gate_part * jax.nn.sigmoid(SILU_SHARPNESS * gate_part))

def reference(mix_rows, mix_gain, w_query, w_key, w_value, key_offset, w_out, out_gain, exp_rows, exp_gain, routes, route_weight, w_gate, w_up, w_down):
    normed = normalize(mix_rows, mix_gain).astype(jnp.bfloat16)
    length = normed.shape[0]
    queries = project(normed, w_query).astype(jnp.float32).reshape(length, ATTENTION_HEADS, HEAD)
    key_rows = project(normed, w_key).astype(jnp.float32).reshape(length, ATTENTION_HEADS, HEAD)
    value_rows = project(normed, w_value).astype(jnp.float32).reshape(length, ATTENTION_HEADS, HEAD)
    offset_values = key_offset.astype(jnp.float32)
    key_index = jnp.arange(length, dtype=jnp.int32)

    def one_block(first_row):
        block_q = lax.dynamic_slice_in_dim(queries, first_row, MIX_ROWS, 0)
        scores = jnp.einsum('thd,shd->hts', block_q, key_rows) / math.sqrt(HEAD) + offset_values[:, None, :]
        query_index = first_row + jnp.arange(MIX_ROWS, dtype=jnp.int32)
        visible = (key_index[None, :] < query_index[:, None])[None]
        weights = stick_weights(scores, visible).astype(jnp.bfloat16)
        weights = lax.optimization_barrier(weights).astype(jnp.float32)
        return jnp.einsum('hts,shd->thd', weights, value_rows)
    starts = jnp.arange(length // MIX_ROWS, dtype=jnp.int32) * MIX_ROWS
    attended = lax.map(one_block, starts).reshape(length, ATTENTION_HEADS * HEAD).astype(jnp.bfloat16)
    mixed_sum = jnp.dot(attended, w_out, preferred_element_type=jnp.float32)
    mix_out = normalize(mixed_sum, out_gain).astype(jnp.bfloat16)
    tokens = exp_rows.shape[0]
    normed_exp = normalize(exp_rows, exp_gain).astype(jnp.bfloat16)
    route_list = routes.reshape(-1).astype(jnp.int32)
    pair_count = route_list.shape[0]
    owners = jnp.arange(pair_count, dtype=jnp.int32) // TOPK
    block_of = owners // EXP_ROWS
    matches = (route_list[:, None] == jnp.arange(EXPERTS, dtype=jnp.int32)[None, :]).astype(jnp.int32)
    grouped = matches.reshape(tokens // EXP_ROWS, EXP_ROWS * TOPK, EXPERTS)
    earlier = (jnp.cumsum(grouped, axis=1) - grouped).reshape(pair_count, EXPERTS)
    slot_index = block_of * CAP + lax.optimization_barrier(jnp.sum(earlier * matches, axis=1))
    table = jnp.full((EXPERTS, tokens // EXP_ROWS * CAP), -1, jnp.int32).at[route_list, slot_index].set(owners)
    piece_count = FF // FF_PART

    def one_expert(operands):
        chosen, gate_weight, up_weight, down_weight = operands
        expert_rows = jnp.where(chosen[:, None] >= 0, normed_exp[jnp.maximum(chosen, 0)], jnp.zeros((), jnp.bfloat16))
        gate_pre = jnp.dot(expert_rows, gate_weight, preferred_element_type=jnp.float32)
        up_pre = jnp.dot(expert_rows, up_weight, preferred_element_type=jnp.float32)
        hidden = gated_units(gate_pre, up_pre).astype(jnp.bfloat16)
        row_total = hidden.shape[0]
        partials = jnp.einsum('spw,pwd->psd', hidden.astype(jnp.float32).reshape(row_total, piece_count, FF_PART), down_weight.astype(jnp.float32).reshape(piece_count, FF_PART, D))
        partials = lax.optimization_barrier(partials.astype(jnp.bfloat16)).astype(jnp.float32)
        return lax.optimization_barrier(jnp.sum(partials, axis=0)).astype(jnp.bfloat16)
    expert_out = lax.map(one_expert, (table, w_gate, w_up, w_down))
    picked = expert_out[route_list, slot_index].astype(jnp.float32).reshape(tokens, TOPK, D)
    exp_out = lax.optimization_barrier(jnp.sum(picked * route_weight.astype(jnp.float32)[:, :, None], axis=1)).astype(jnp.bfloat16)
    return (mix_out, exp_out)
```

```python
import math

import jax
import jax.numpy as jnp
from jax import lax
from jax.experimental import pallas as pl
from jax.experimental.pallas import tpu as pltpu
from jax.sharding import Mesh
from jax.sharding import PartitionSpec as P

EP = ("ep_0", "ep_1")
TP = ("tp_0", "tp_1")

EPSILON = 1e-06
CLAMP_LIMIT = 7.0
SILU_SHARPNESS = 1.702
LOG2E = 1.4426950408889634
PAD = 16
UNROLL = 4


def dot(a, b, dims=((1,), (0,)), precision=None):
    return lax.dot_general(
        a, b, (dims, ((), ())), precision=precision, preferred_element_type=jnp.float32
    )


def row_factor(total, width):
    return lax.rsqrt(total / width + EPSILON)


def prepare_kernel(
    routes, weight, rows, mix_rows, gain, w_query, w_key, w_value, queries, payload, table
):
    top, tokens = routes.shape
    slots = table.shape[0]
    across, _, _ = payload.shape
    positions = mix_rows.shape[0]
    along = slots // (across * PAD)
    capacity = PAD
    slot = lax.broadcasted_iota(jnp.int32, (slots, tokens), 0)
    expert_of = slot // capacity
    place_of = slot - expert_of * capacity
    named = jnp.zeros((slots, tokens), jnp.float32)
    scale = jnp.zeros((slots, tokens), jnp.float32)
    for k in range(top):
        here = routes[k : k + 1, :] == expert_of
        named = jnp.where(here, 1.0, named)
        scale = jnp.where(here, weight[k : k + 1, :], scale)
    earlier = lax.broadcasted_iota(jnp.int32, (tokens, tokens), 0) < lax.broadcasted_iota(
        jnp.int32, (tokens, tokens), 1
    )
    earlier = jnp.where(earlier, 1.0, 0.0).astype(jnp.bfloat16)
    place = dot(named.astype(jnp.bfloat16), earlier)
    mine = (named > 0.0) & (place == place_of.astype(jnp.float32))
    table[...] = jnp.where(mine, scale, 0.0)
    chosen = jnp.where(mine, 1.0, 0.0).astype(jnp.bfloat16)
    outgoing = dot(chosen, rows[...]).astype(payload.dtype)
    for x in range(across):
        for z in range(along):
            at = (z * across + x) * capacity
            to = positions + z * capacity
            payload[x, to : to + capacity, :] = outgoing[at : at + capacity]

    numbers = mix_rows[...].astype(jnp.float32)
    factor = row_factor(jnp.sum(numbers * numbers, axis=1, keepdims=True), numbers.shape[1])
    normed = (numbers * factor * gain[...][None].astype(jnp.float32)).astype(jnp.bfloat16)
    queries[...] = dot(normed, w_query[...], ((1,), (1,))).astype(jnp.bfloat16)
    keys = dot(normed, w_key[...], ((1,), (1,)))
    values = dot(normed, w_value[...], ((1,), (1,)))
    pairs = jnp.concatenate([keys, values], axis=1).astype(payload.dtype)
    for x in range(across):
        payload[x, :positions, :] = pairs


def columns_kernel(w_down, w_out, out):
    parts, _, width = out.shape
    hidden = w_down.shape[1]
    for k in range(parts):
        at = slice(k * width, (k + 1) * width)
        out[k, :hidden, :] = w_down[0, :, at]
        out[k, hidden:, :] = w_out[:, at]


def attend_kernel(own_ref, queries, pairs, offsets, out):
    own = own_ref[0]
    rows, head = queries.shape
    q = queries[...]
    visible = lax.broadcasted_iota(jnp.int32, (rows, rows), 1) < lax.broadcasted_iota(
        jnp.int32, (rows, rows), 0
    )
    after = jnp.where(visible, -1.0, 0.0).astype(jnp.bfloat16)

    def front(j, diagonal):
        pair = pairs[j]
        offset = offsets[:, pl.ds(pl.multiple_of(j * rows, rows), rows)]
        s = dot(q, pair[:, :head], ((1,), (1,)))
        s = s * (LOG2E / math.sqrt(head)) + offset * LOG2E
        soft = jnp.log2(1.0 + jnp.exp2(-jnp.abs(s)))
        take = jnp.minimum(s, 0.0) - soft
        cost = jnp.maximum(s, 0.0) + soft
        if diagonal:
            cost = jnp.where(visible, cost, 0.0)
        inside = dot(cost.astype(jnp.bfloat16), after)
        return take + inside, inside[:, :1] - cost[:, :1], pair[:, head:]

    def back(ahead, state, diagonal):
        later, acc = state
        exponent, total, values = ahead
        w = jnp.exp2(exponent + later)
        if diagonal:
            w = jnp.where(visible, w, 0.0)
        return later + total, acc + dot(w.astype(jnp.bfloat16), values)

    def group(j, count, state):
        ahead = [front(j - i, False) for i in range(count)]
        for one in ahead:
            state = back(one, state, False)
        return state

    state = (jnp.zeros((rows, 1), jnp.float32), jnp.zeros((rows, head), jnp.float32))
    state = back(front(own, True), state, True)
    rest = own % UNROLL
    state = lax.fori_loop(0, rest, lambda i, c: group(own - 1 - i, 1, c), state)
    state = lax.fori_loop(
        0, own // UNROLL, lambda i, c: group(own - 1 - rest - i * UNROLL, UNROLL, c), state
    )
    half = rows // 2
    acc = state[1].astype(out.dtype)
    out[...] = jnp.concatenate([acc[:half], acc[half:]], axis=1)


def mix_columns_kernel(attended, weights, out):
    parts, half, width = attended.shape
    head = width // 2
    skip = weights.shape[1] - head
    side = jnp.concatenate([weights[k, skip:, :] for k in range(parts)], axis=0)
    top = jnp.concatenate([attended[k][:, :head] for k in range(parts)], axis=1)
    low = jnp.concatenate([attended[k][:, head:] for k in range(parts)], axis=1)
    out[:half, :] = dot(top, side).astype(out.dtype)
    out[half:, :] = dot(low, side).astype(out.dtype)


def mix_norm_kernel(core_ref, mine, theirs, gain, out):
    core = core_ref[0]
    groups, rows, width = mine.shape
    total = jnp.zeros((rows, width), jnp.float32)
    for k in range(groups):
        for side in (mine, theirs):
            numbers = side[k].astype(jnp.float32)
            total = total + numbers * numbers
    factor = row_factor(jnp.sum(total, axis=1, keepdims=True), 2 * groups * width)
    scale = gain[...].astype(jnp.float32)[None]
    first = core == 0
    for k in range(groups):
        pair = (mine[k].astype(jnp.float32), theirs[k].astype(jnp.float32))
        for which in range(2):
            at = slice((2 * k + which) * width, (2 * k + which + 1) * width)
            numbers = jnp.where(first, pair[which], pair[1 - which])
            out[:, at] = (numbers * factor * scale[:, at]).astype(out.dtype)


def expert_kernel(core_ref, mine, theirs, w_gate, w_up, out, normed):
    core = core_ref[0]
    groups, padded, width = mine.shape
    rows = padded - PAD
    total = jnp.zeros((rows, width), jnp.float32)
    for k in range(groups):
        for side in (mine, theirs):
            numbers = side[k, :rows, :].astype(jnp.float32)
            total = total + numbers * numbers
    factor = row_factor(jnp.sum(total, axis=1, keepdims=True), 2 * groups * width)
    for k in range(groups):
        for side, which in ((mine, core), (theirs, 1 - core)):
            at = pl.ds(pl.multiple_of((2 * k + which) * width, width), width)
            gain = side[k, rows : rows + 1, :].astype(jnp.float32)
            numbers = side[k, :rows, :].astype(jnp.float32) * factor * gain
            normed[:, at] = numbers.astype(jnp.bfloat16)
    gate = jnp.minimum(dot(normed[...], w_gate[0]), CLAMP_LIMIT)
    up = jnp.clip(dot(normed[...], w_up[0]), -CLAMP_LIMIT, CLAMP_LIMIT)
    hidden = (up + 1.0) * (gate * jax.nn.sigmoid(SILU_SHARPNESS * gate))
    out[...] = hidden.astype(out.dtype)


def down_kernel(hidden, weights, out):
    parts, _, width = hidden.shape
    total = jnp.zeros(out.shape, jnp.float32)
    for k in range(0, parts, 2):
        both = jnp.concatenate([hidden[k], hidden[k + 1]], axis=1)
        side = jnp.concatenate([weights[k, :width, :], weights[k + 1, :width, :]], axis=0)
        total = total + dot(both, side)
    out[...] = total.astype(out.dtype)


def combine_kernel(table, returned, out):
    scale = table[...]
    rows = returned[...]
    total = jnp.zeros(out.shape, jnp.float32)
    for _ in range(3):
        part = scale.astype(jnp.bfloat16)
        total = total + dot(part, rows, ((0,), (0,)))
        scale = scale - part.astype(jnp.float32)
    out[...] = total.astype(out.dtype)


def call(body, outs, *args, scalars=0, **kwargs):
    spaces = [pltpu.SMEM] * scalars + [pltpu.VMEM] * (len(args) - scalars)
    specs = [pl.BlockSpec(memory_space=space) for space in spaces]
    return pl.pallas_call(body, out_shape=outs, in_specs=specs, **kwargs)(*args)


def stacked(value, axis):
    copies = jnp.broadcast_to(value, (lax.axis_size(axis), *value.shape))
    return exchanged(copies, axis)


def exchanged(value, axis):
    return lax.all_to_all(value, axis, 0, 0, tiled=True)


def from_partner(value):
    return lax.ppermute(value, "tp_1", [(0, 1), (1, 0)])


def on_device(
    mix_rows,
    mix_gain,
    w_query,
    w_key,
    w_value,
    key_offset,
    w_out,
    out_gain,
    exp_rows,
    exp_gain,
    routes,
    route_weight,
    w_gate,
    w_up,
    w_down,
):
    bf16 = jnp.bfloat16
    shape = jax.ShapeDtypeStruct
    ep_count = lax.axis_size(EP)
    tp_count = lax.axis_size(TP)
    tokens, top = routes.shape
    part = exp_rows.shape[1]
    experts = ep_count * w_gate.shape[0]
    capacity = 4 * tokens * top // (3 * experts)
    slots = experts * capacity
    rows = mix_rows.shape[0]
    head = w_query.shape[0]
    model = mix_rows.shape[1]
    own = lax.axis_index(EP).astype(jnp.int32)[None]
    core = lax.axis_index("tp_1").astype(jnp.int32)[None]

    across = lax.axis_size("ep_1")
    height = rows + slots // across
    queries, payload, table = call(
        prepare_kernel,
        (
            shape((rows, head), bf16),
            shape((across, height, part), bf16),
            shape((slots, tokens), jnp.float32),
        ),
        routes.T,
        route_weight.T,
        exp_rows,
        mix_rows,
        mix_gain,
        w_query,
        w_key,
        w_value,
    )
    payload = exchanged(payload, "ep_1")
    pairs = payload[:, :rows]
    every_pair = lax.all_gather(pairs, "ep_0", axis=0, tiled=True)
    outgoing = payload[:, rows:].reshape(across, -1, capacity, part).swapaxes(0, 1)
    arrived = exchanged(outgoing, "ep_0").reshape(slots, part)
    gain_rows = jnp.broadcast_to(exp_gain[None], (PAD, part))
    mine = stacked(jnp.concatenate([arrived, gain_rows], axis=0), "tp_0")

    columns = call(
        columns_kernel,
        shape((tp_count, w_down.shape[1] + head, model // tp_count), bf16),
        w_down,
        w_out,
    )
    columns = exchanged(columns, TP)

    hidden = call(
        expert_kernel,
        shape((slots, w_gate.shape[2]), bf16),
        core,
        mine,
        from_partner(mine),
        w_gate,
        w_up,
        scalars=1,
        scratch_shapes=[pltpu.VMEM((slots, model), bf16)],
    )
    every_hidden = lax.all_gather(hidden, TP, axis=0)
    expert_out = call(down_kernel, shape((slots, part), bf16), every_hidden, columns)
    returned = exchanged(expert_out, EP)
    exp_out = call(combine_kernel, shape((tokens, part), bf16), table, returned)

    attended = call(
        attend_kernel,
        shape((rows // 2, 2 * head), bf16),
        own,
        queries,
        every_pair,
        key_offset,
        scalars=1,
    )
    every_head = lax.all_gather(attended, TP, axis=0)
    own_columns = call(
        mix_columns_kernel, shape((rows, model // tp_count), bf16), every_head, columns
    )
    mine = stacked(own_columns, "tp_0")
    mix_out = call(
        mix_norm_kernel,
        shape((rows, model), bf16),
        core,
        mine,
        from_partner(mine),
        out_gain,
        scalars=1,
    )
    return (mix_out, exp_out)


def solution(mesh):
    torus = Mesh(mesh.devices.reshape(8, 4, 8, 2), ("ep_0", "ep_1", "tp_0", "tp_1"))
    in_specs = (
        P(EP, None),
        P(),
        P(TP, None),
        P(TP, None),
        P(TP, None),
        P(TP, None),
        P(TP, None),
        P(),
        P(EP, TP),
        P(TP),
        P(EP, None),
        P(EP, None),
        P(EP, None, TP),
        P(EP, None, TP),
        P(EP, TP, None),
    )
    out_specs = (P(EP, None), P(EP, TP))

    def step(*args):
        return on_device(*args)

    step = jax.shard_map(
        step, mesh=torus, in_specs=in_specs, out_specs=out_specs, check_vma=False
    )
    return step
```

```python
import math

import jax
import jax.numpy as jnp
from jax import lax
from jax.experimental import pallas as pl
from jax.experimental.pallas import tpu as pltpu
from jax.sharding import Mesh
from jax.sharding import PartitionSpec as P

EP = ("ep_0", "ep_1")
TP = ("tp_0", "tp_1")

EPSILON = 1e-06
CLAMP_LIMIT = 7.0
SILU_SHARPNESS = 1.702
LOG2E = 1.4426950408889634
PAD = 16


def dot(a, b, dims=((1,), (0,)), precision=None):
    return lax.dot_general(
        a, b, (dims, ((), ())), precision=precision, preferred_element_type=jnp.float32
    )


def row_factor(total, width):
    return lax.rsqrt(total / width + EPSILON)


def prepare_kernel(
    routes, weight, rows, mix_rows, gain, w_query, w_key, w_value, queries, payload, table
):
    top, tokens = routes.shape
    slots = table.shape[0]
    across, _, _ = payload.shape
    positions = mix_rows.shape[0]
    along = slots // (across * PAD)
    capacity = PAD
    slot = lax.broadcasted_iota(jnp.int32, (slots, tokens), 0)
    expert_of = slot // capacity
    place_of = slot - expert_of * capacity
    named = jnp.zeros((slots, tokens), jnp.float32)
    scale = jnp.zeros((slots, tokens), jnp.float32)
    for k in range(top):
        here = routes[k : k + 1, :] == expert_of
        named = jnp.where(here, 1.0, named)
        scale = jnp.where(here, weight[k : k + 1, :], scale)
    earlier = lax.broadcasted_iota(jnp.int32, (tokens, tokens), 0) < lax.broadcasted_iota(
        jnp.int32, (tokens, tokens), 1
    )
    earlier = jnp.where(earlier, 1.0, 0.0).astype(jnp.bfloat16)
    place = dot(named.astype(jnp.bfloat16), earlier)
    mine = (named > 0.0) & (place == place_of.astype(jnp.float32))
    table[...] = jnp.where(mine, scale, 0.0)
    chosen = jnp.where(mine, 1.0, 0.0).astype(jnp.bfloat16)
    outgoing = dot(chosen, rows[...]).astype(payload.dtype)
    for x in range(across):
        for z in range(along):
            at = (z * across + x) * capacity
            to = positions + z * capacity
            payload[x, to : to + capacity, :] = outgoing[at : at + capacity]

    numbers = mix_rows[...].astype(jnp.float32)
    factor = row_factor(jnp.sum(numbers * numbers, axis=1, keepdims=True), numbers.shape[1])
    normed = (numbers * factor * gain[...][None].astype(jnp.float32)).astype(jnp.bfloat16)
    half = positions // 2
    asked = dot(normed, w_query[...], ((1,), (1,))).astype(jnp.bfloat16)
    queries[...] = jnp.concatenate([asked[:half], asked[half:]], axis=1)
    keys = dot(normed, w_key[...], ((1,), (1,)))
    values = dot(normed, w_value[...], ((1,), (1,)))
    pairs = jnp.concatenate([keys, values], axis=1).astype(payload.dtype)
    for x in range(across):
        payload[x, :positions, :] = pairs


def columns_kernel(w_down, w_out, out):
    parts, _, width = out.shape
    hidden = w_down.shape[1]
    for k in range(parts):
        at = slice(k * width, (k + 1) * width)
        out[k, :hidden, :] = w_down[0, :, at]
        out[k, hidden:, :] = w_out[:, at]


def relay_kernel(payload, queries, out):
    across = payload.shape[0]
    along = out.shape[0]
    half = queries.shape[0]
    positions = 2 * half
    own = queries[...]
    for z in range(along):
        at = slice(positions + z * PAD, positions + (z + 1) * PAD)
        for x in range(across):
            out[z, x * PAD : (x + 1) * PAD, :] = payload[x, at, :]
        out[z, across * PAD :, :] = own


def identity(size):
    row = lax.broadcasted_iota(jnp.int32, (size, size), 0)
    return jnp.where(row == lax.broadcasted_iota(jnp.int32, (size, size), 1), 1.0, 0.0)


def attend_kernel(where_ref, payload, asked, offsets, out):
    z, x = where_ref[0], where_ref[1]
    across = payload.shape[0]
    along = asked.shape[0]
    half = asked.shape[1] - across * PAD
    rows = 2 * half
    head = asked.shape[2] // 2
    visible = lax.broadcasted_iota(jnp.int32, (rows, rows), 1) < lax.broadcasted_iota(
        jnp.int32, (rows, rows), 0
    )
    after = jnp.where(visible, -1.0, 0.0).astype(jnp.bfloat16)
    turn = identity(rows).astype(jnp.bfloat16)

    def front(q, j, diagonal):
        pair = payload[j, :rows, :]
        at = pl.multiple_of((z * across + j) * rows, rows)
        s = dot(q, pair[:, :head], ((1,), (1,)))
        s = s * (LOG2E / math.sqrt(head)) + offsets[:, pl.ds(at, rows)] * LOG2E
        soft = jnp.log2(1.0 + jnp.exp2(-jnp.abs(s)))
        take = jnp.minimum(s, 0.0) - soft
        cost = jnp.maximum(s, 0.0) + soft
        if diagonal:
            cost = jnp.where(visible, cost, 0.0)
        inside = dot(cost.astype(jnp.bfloat16), after)
        return take + inside, inside[:, :1] - cost[:, :1], pair[:, head:]

    def back(ahead, state, diagonal):
        later, acc = state
        exponent, total, values = ahead
        w = jnp.exp2(exponent + later)
        if diagonal:
            w = jnp.where(visible, w, 0.0)
        return later + total, acc + dot(w.astype(jnp.bfloat16), values)

    def asked_by(block):
        both = asked[block, across * PAD :, :]
        return jnp.concatenate([both[:, :head], both[:, head:]], axis=0)

    def send(block, state):
        later, acc = state
        acc = acc.astype(out.dtype)
        out[block, :half, :] = jnp.concatenate([acc[:half], acc[half:]], axis=1)
        high = later.astype(jnp.bfloat16)
        low = (later - high.astype(jnp.float32)).astype(jnp.bfloat16)
        wide = (rows, PAD // 2)
        parts = [jnp.broadcast_to(high, wide), jnp.broadcast_to(low, wide)]
        parts = dot(jnp.concatenate(parts, axis=1), turn, ((0,), (0,))).astype(out.dtype)
        out[block, half : half + PAD, :] = parts[:, :half]
        out[block, half + PAD :, :] = parts[:, half:]

    start = (jnp.zeros((rows, 1), jnp.float32), jnp.zeros((rows, head), jnp.float32))

    def nothing(block, carry):
        out[block] = jnp.zeros(out.shape[1:], out.dtype)
        return carry

    def everything(block, carry):
        q = asked_by(block)
        state = start
        ahead = [front(q, across - 1 - i, False) for i in range(across)]
        for one in ahead:
            state = back(one, state, False)
        send(block, state)
        return carry

    lax.fori_loop(0, z, nothing, 0)
    q = asked_by(z)
    state = back(front(q, x, True), start, True)
    state = lax.fori_loop(0, x, lambda i, c: back(front(q, x - 1 - i, False), c, False), state)
    send(z, state)
    lax.fori_loop(z + 1, along, everything, 0)


def gather_kernel(partial, out):
    along, _, width = partial.shape
    half, head = width, width // 2
    rows = 2 * half
    turn = identity(rows).astype(jnp.bfloat16)
    later = jnp.zeros((rows, 1), jnp.float32)
    total = jnp.zeros((rows, head), jnp.float32)
    for g in range(along - 1, -1, -1):
        both = partial[g, :half, :].astype(jnp.float32)
        both = jnp.concatenate([both[:, :head], both[:, head:]], axis=0)
        total = total + jnp.exp2(later) * both
        parts = [partial[g, half : half + PAD, :], partial[g, half + PAD :, :]]
        parts = dot(turn, jnp.concatenate(parts, axis=1), ((1,), (1,)))
        later = later + (parts[:, :1] + parts[:, PAD // 2 : PAD // 2 + 1])
    total = total.astype(out.dtype)
    out[...] = jnp.concatenate([total[:half], total[half:]], axis=1)


def mix_columns_kernel(attended, weights, out):
    parts, half, width = attended.shape
    head = width // 2
    skip = weights.shape[1] - head
    side = jnp.concatenate([weights[k, skip:, :] for k in range(parts)], axis=0)
    top = jnp.concatenate([attended[k][:, :head] for k in range(parts)], axis=1)
    low = jnp.concatenate([attended[k][:, head:] for k in range(parts)], axis=1)
    top = dot(top, side).astype(out.dtype)
    low = dot(low, side).astype(out.dtype)
    for copy in range(out.shape[0]):
        out[copy, :half, :] = top
        out[copy, half:, :] = low


def mix_norm_kernel(core_ref, mine, theirs, gain, out):
    core = core_ref[0]
    groups, rows, width = mine.shape
    total = jnp.zeros((rows, width), jnp.float32)
    for k in range(groups):
        for side in (mine, theirs):
            numbers = side[k].astype(jnp.float32)
            total = total + numbers * numbers
    factor = row_factor(jnp.sum(total, axis=1, keepdims=True), 2 * groups * width)
    scale = gain[...].astype(jnp.float32)[None]
    first = core == 0
    for k in range(groups):
        pair = (mine[k].astype(jnp.float32), theirs[k].astype(jnp.float32))
        for which in range(2):
            at = slice((2 * k + which) * width, (2 * k + which + 1) * width)
            numbers = jnp.where(first, pair[which], pair[1 - which])
            out[:, at] = (numbers * factor * scale[:, at]).astype(out.dtype)


def expert_kernel(arrived, w_gate, w_up, out, scaled, both):
    parts, padded, width = arrived.shape
    rows = padded - PAD
    hidden = w_gate.shape[2]
    both[:, :hidden] = w_gate[0]
    both[:, hidden:] = w_up[0]
    total = jnp.zeros((rows, width), jnp.float32)
    for k in range(parts):
        numbers = arrived[k, :rows, :].astype(jnp.float32)
        total = total + numbers * numbers
        gain = arrived[k, rows : rows + 1, :].astype(jnp.float32)
        scaled[:, k * width : (k + 1) * width] = (numbers * gain).astype(jnp.bfloat16)
    factor = row_factor(jnp.sum(total, axis=1, keepdims=True), parts * width)
    pre = dot(scaled[...], both[...]) * factor
    gate = jnp.minimum(pre[:, :hidden], CLAMP_LIMIT)
    up = jnp.clip(pre[:, hidden:], -CLAMP_LIMIT, CLAMP_LIMIT)
    units = (up + 1.0) * (gate * jax.nn.sigmoid(SILU_SHARPNESS * gate))
    out[...] = units.astype(out.dtype)


def down_kernel(hidden, weights, out):
    parts, _, width = hidden.shape
    total = jnp.zeros(out.shape, jnp.float32)
    for k in range(0, parts, 2):
        both = jnp.concatenate([hidden[k], hidden[k + 1]], axis=1)
        side = jnp.concatenate([weights[k, :width, :], weights[k + 1, :width, :]], axis=0)
        total = total + dot(both, side)
    out[...] = total.astype(out.dtype)


def combine_kernel(table, returned, out):
    scale = table[...]
    rows = returned[...]
    total = jnp.zeros(out.shape, jnp.float32)
    for _ in range(3):
        part = scale.astype(jnp.bfloat16)
        total = total + dot(part, rows, ((0,), (0,)))
        scale = scale - part.astype(jnp.float32)
    out[...] = total.astype(out.dtype)


def call(body, outs, *args, scalars=0, **kwargs):
    spaces = [pltpu.SMEM] * scalars + [pltpu.VMEM] * (len(args) - scalars)
    specs = [pl.BlockSpec(memory_space=space) for space in spaces]
    return pl.pallas_call(body, out_shape=outs, in_specs=specs, **kwargs)(*args)


def exchanged(value, axis):
    return lax.all_to_all(value, axis, 0, 0, tiled=True)


def from_partner(value):
    return lax.ppermute(value, "tp_1", [(0, 1), (1, 0)])


def on_device(
    mix_rows,
    mix_gain,
    w_query,
    w_key,
    w_value,
    key_offset,
    w_out,
    out_gain,
    exp_rows,
    exp_gain,
    routes,
    route_weight,
    w_gate,
    w_up,
    w_down,
):
    bf16 = jnp.bfloat16
    shape = jax.ShapeDtypeStruct
    ep_count = lax.axis_size(EP)
    tp_count = lax.axis_size(TP)
    tokens, top = routes.shape
    part = exp_rows.shape[1]
    experts = ep_count * w_gate.shape[0]
    capacity = 4 * tokens * top // (3 * experts)
    slots = experts * capacity
    rows = mix_rows.shape[0]
    head = w_query.shape[0]
    model = mix_rows.shape[1]
    own = jnp.stack([lax.axis_index("ep_0"), lax.axis_index("ep_1")]).astype(jnp.int32)
    core = lax.axis_index("tp_1").astype(jnp.int32)[None]

    across = lax.axis_size("ep_1")
    along = lax.axis_size("ep_0")
    half = rows // 2
    queries, payload, table = call(
        prepare_kernel,
        (
            shape((half, 2 * head), bf16),
            shape((across, rows + along * capacity, part), bf16),
            shape((slots, tokens), jnp.float32),
        ),
        routes.T,
        route_weight.T,
        exp_rows,
        mix_rows,
        mix_gain,
        w_query,
        w_key,
        w_value,
    )
    payload = exchanged(payload, "ep_1")
    asked = call(
        relay_kernel, shape((along, across * capacity + half, part), bf16), payload, queries
    )
    asked = exchanged(asked, "ep_0")
    arrived = asked[:, : across * capacity].reshape(slots, part)
    gain_rows = jnp.broadcast_to(exp_gain[None], (PAD, part))
    every_row = jnp.concatenate([arrived, gain_rows], axis=0)
    every_row = lax.all_gather(every_row, TP, axis=0)

    columns = call(
        columns_kernel,
        shape((tp_count, w_down.shape[1] + head, model // tp_count), bf16),
        w_down,
        w_out,
    )
    columns = exchanged(columns, TP)

    partial = call(
        attend_kernel,
        shape((along, half + 2 * PAD, 2 * head), bf16),
        own,
        payload,
        asked,
        key_offset,
        scalars=1,
    )
    partial = exchanged(partial, "ep_0")
    attended = call(gather_kernel, shape((half, 2 * head), bf16), partial)

    units = w_gate.shape[2]
    hidden = call(
        expert_kernel,
        shape((slots, units), bf16),
        every_row,
        w_gate,
        w_up,
        scratch_shapes=[
            pltpu.VMEM((slots, model), bf16),
            pltpu.VMEM((model, 2 * units), bf16),
        ],
    )
    every_hidden = lax.all_gather(hidden, TP, axis=0)
    expert_out = call(down_kernel, shape((slots, part), bf16), every_hidden, columns)
    returned = exchanged(expert_out, EP)
    exp_out = call(combine_kernel, shape((tokens, part), bf16), table, returned)

    every_head = lax.all_gather(attended, TP, axis=0)
    own_columns = call(
        mix_columns_kernel,
        shape((tp_count // 2, rows, model // tp_count), bf16),
        every_head,
        columns,
    )
    mine = exchanged(own_columns, "tp_0")
    mix_out = call(
        mix_norm_kernel,
        shape((rows, model), bf16),
        core,
        mine,
        from_partner(mine),
        out_gain,
        scalars=1,
    )
    return (mix_out, exp_out)


def solution(mesh):
    torus = Mesh(mesh.devices.reshape(8, 4, 8, 2), ("ep_0", "ep_1", "tp_0", "tp_1"))
    in_specs = (
        P(EP, None),
        P(),
        P(TP, None),
        P(TP, None),
        P(TP, None),
        P(TP, None),
        P(TP, None),
        P(),
        P(EP, TP),
        P(TP),
        P(EP, None),
        P(EP, None),
        P(EP, None, TP),
        P(EP, None, TP),
        P(EP, TP, None),
    )
    out_specs = (P(EP, None), P(EP, TP))

    def step(*args):
        return on_device(*args)

    step = jax.shard_map(
        step, mesh=torus, in_specs=in_specs, out_specs=out_specs, check_vma=False
    )
    return step
```

```python
import math

import jax
import jax.numpy as jnp
from jax import lax
from jax.experimental import pallas as pl
from jax.experimental.pallas import tpu as pltpu
from jax.sharding import Mesh
from jax.sharding import PartitionSpec as P

EP = ("ep_0", "ep_1")
TP = ("tp_0", "tp_1")

EPSILON = 1e-06
CLAMP_LIMIT = 7.0
SILU_SHARPNESS = 1.702
LOG2E = 1.4426950408889634
PAD = 16


def dot(a, b, dims=((1,), (0,)), precision=None):
    return lax.dot_general(
        a, b, (dims, ((), ())), precision=precision, preferred_element_type=jnp.float32
    )


def row_factor(total, width):
    return lax.rsqrt(total / width + EPSILON)


def prepare_kernel(
    routes, weight, rows, mix_rows, gain, w_query, w_key, w_value, asked, pairs, outgoing, table
):
    top, tokens = routes.shape
    slots = table.shape[0]
    slot = lax.broadcasted_iota(jnp.int32, (slots, tokens), 0)
    expert_of = slot // PAD
    place_of = slot - expert_of * PAD
    named = jnp.zeros((slots, tokens), jnp.float32)
    scale = jnp.zeros((slots, tokens), jnp.float32)
    for k in range(top):
        here = routes[k : k + 1, :] == expert_of
        named = jnp.where(here, 1.0, named)
        scale = jnp.where(here, weight[k : k + 1, :], scale)
    earlier = lax.broadcasted_iota(jnp.int32, (tokens, tokens), 0) < lax.broadcasted_iota(
        jnp.int32, (tokens, tokens), 1
    )
    earlier = jnp.where(earlier, 1.0, 0.0).astype(jnp.bfloat16)
    place = dot(named.astype(jnp.bfloat16), earlier)
    mine = (named > 0.0) & (place == place_of.astype(jnp.float32))
    table[...] = jnp.where(mine, scale, 0.0)
    chosen = jnp.where(mine, 1.0, 0.0).astype(jnp.bfloat16)
    outgoing[...] = dot(chosen, rows[...]).astype(outgoing.dtype)

    numbers = mix_rows[...].astype(jnp.float32)
    factor = row_factor(jnp.sum(numbers * numbers, axis=1, keepdims=True), numbers.shape[1])
    normed = (numbers * factor * gain[...][None].astype(jnp.float32)).astype(jnp.bfloat16)
    queries = dot(normed, w_query[...], ((1,), (1,))).astype(asked.dtype)
    half = queries.shape[0] // 2
    queries = jnp.concatenate([queries[:half], queries[half:]], axis=1)
    for copy in range(asked.shape[0]):
        asked[copy] = queries
    keys = dot(normed, w_key[...], ((1,), (1,)))
    values = dot(normed, w_value[...], ((1,), (1,)))
    pairs[...] = jnp.concatenate([keys, values], axis=1).astype(pairs.dtype)


def columns_kernel(w_down, w_out, out):
    parts, _, width = out.shape
    hidden = w_down.shape[1]
    for k in range(parts):
        at = slice(k * width, (k + 1) * width)
        out[k, :hidden, :] = w_down[0, :, at]
        out[k, hidden:, :] = w_out[:, at]


def identity(size):
    row = lax.broadcasted_iota(jnp.int32, (size, size), 0)
    return jnp.where(row == lax.broadcasted_iota(jnp.int32, (size, size), 1), 1.0, 0.0)


def attend_kernel(where_ref, pairs, asked, offsets, out):
    z, x = where_ref[0], where_ref[1]
    across = pairs.shape[0]
    along, half = asked.shape[:2]
    rows = 2 * half
    head = asked.shape[2] // 2
    visible = lax.broadcasted_iota(jnp.int32, (rows, rows), 1) < lax.broadcasted_iota(
        jnp.int32, (rows, rows), 0
    )
    after = jnp.where(visible, -1.0, 0.0).astype(jnp.bfloat16)
    turn = identity(rows).astype(jnp.bfloat16)

    def front(q, j, diagonal):
        pair = pairs[j]
        at = pl.multiple_of((z * across + j) * rows, rows)
        s = dot(q, pair[:, :head], ((1,), (1,)))
        s = s * (LOG2E / math.sqrt(head)) + offsets[:, pl.ds(at, rows)] * LOG2E
        soft = jnp.log2(1.0 + jnp.exp2(-jnp.abs(s)))
        take = jnp.minimum(s, 0.0) - soft
        cost = jnp.maximum(s, 0.0) + soft
        if diagonal:
            cost = jnp.where(visible, cost, 0.0)
        inside = dot(cost.astype(jnp.bfloat16), after)
        return take + inside, inside[:, :1] - cost[:, :1], pair[:, head:]

    def back(ahead, state, diagonal):
        later, acc = state
        exponent, total, values = ahead
        w = jnp.exp2(exponent + later)
        if diagonal:
            w = jnp.where(visible, w, 0.0)
        return later + total, acc + dot(w.astype(jnp.bfloat16), values)

    def asked_by(block):
        both = asked[block]
        return jnp.concatenate([both[:, :head], both[:, head:]], axis=0)

    def send(block, state):
        later, acc = state
        acc = acc.astype(out.dtype)
        out[block, :half, :] = jnp.concatenate([acc[:half], acc[half:]], axis=1)
        high = later.astype(jnp.bfloat16)
        low = (later - high.astype(jnp.float32)).astype(jnp.bfloat16)
        wide = (rows, PAD // 2)
        parts = [jnp.broadcast_to(high, wide), jnp.broadcast_to(low, wide)]
        parts = dot(jnp.concatenate(parts, axis=1), turn, ((0,), (0,))).astype(out.dtype)
        out[block, half : half + PAD, :] = parts[:, :half]
        out[block, half + PAD :, :] = parts[:, half:]

    start = (jnp.zeros((rows, 1), jnp.float32), jnp.zeros((rows, head), jnp.float32))

    def nothing(block, carry):
        out[block] = jnp.zeros(out.shape[1:], out.dtype)
        return carry

    def everything(block, carry):
        q = asked_by(block)
        state = start
        ahead = [front(q, across - 1 - i, False) for i in range(across)]
        for one in ahead:
            state = back(one, state, False)
        send(block, state)
        return carry

    lax.fori_loop(0, z, nothing, 0)
    q = asked_by(z)
    state = back(front(q, x, True), start, True)
    state = lax.fori_loop(0, x, lambda i, c: back(front(q, x - 1 - i, False), c, False), state)
    send(z, state)
    lax.fori_loop(z + 1, along, everything, 0)


def gather_kernel(partial, out):
    along, _, width = partial.shape
    half, head = width, width // 2
    rows = 2 * half
    turn = identity(rows).astype(jnp.bfloat16)
    later = jnp.zeros((rows, 1), jnp.float32)
    total = jnp.zeros((rows, head), jnp.float32)
    for g in range(along - 1, -1, -1):
        both = partial[g, :half, :].astype(jnp.float32)
        both = jnp.concatenate([both[:, :head], both[:, head:]], axis=0)
        total = total + jnp.exp2(later) * both
        parts = [partial[g, half : half + PAD, :], partial[g, half + PAD :, :]]
        parts = dot(turn, jnp.concatenate(parts, axis=1), ((1,), (1,)))
        later = later + (parts[:, :1] + parts[:, PAD // 2 : PAD // 2 + 1])
    total = total.astype(out.dtype)
    out[...] = jnp.concatenate([total[:half], total[half:]], axis=1)


def mix_columns_kernel(attended, weights, out):
    parts, half, width = attended.shape
    head = width // 2
    skip = weights.shape[1] - head
    side = jnp.concatenate([weights[k, skip:, :] for k in range(parts)], axis=0)
    top = jnp.concatenate([attended[k][:, :head] for k in range(parts)], axis=1)
    low = jnp.concatenate([attended[k][:, head:] for k in range(parts)], axis=1)
    top = dot(top, side).astype(out.dtype)
    low = dot(low, side).astype(out.dtype)
    for copy in range(out.shape[0]):
        out[copy, :half, :] = top
        out[copy, half:, :] = low


def mix_norm_kernel(core_ref, mine, theirs, gain, out):
    core = core_ref[0]
    groups, rows, width = mine.shape
    total = jnp.zeros((rows, width), jnp.float32)
    for k in range(groups):
        for side in (mine, theirs):
            numbers = side[k].astype(jnp.float32)
            total = total + numbers * numbers
    factor = row_factor(jnp.sum(total, axis=1, keepdims=True), 2 * groups * width)
    scale = gain[...].astype(jnp.float32)[None]
    first = core == 0
    for k in range(groups):
        pair = (mine[k].astype(jnp.float32), theirs[k].astype(jnp.float32))
        for which in range(2):
            at = slice((2 * k + which) * width, (2 * k + which + 1) * width)
            numbers = jnp.where(first, pair[which], pair[1 - which])
            out[:, at] = (numbers * factor * scale[:, at]).astype(out.dtype)


def expert_kernel(arrived, w_gate, w_up, out, scaled, both):
    parts, padded, width = arrived.shape
    rows = padded - PAD
    hidden = w_gate.shape[2]
    both[:, :hidden] = w_gate[0]
    both[:, hidden:] = w_up[0]
    total = jnp.zeros((rows, width), jnp.float32)
    for k in range(parts):
        numbers = arrived[k, :rows, :].astype(jnp.float32)
        total = total + numbers * numbers
        gain = arrived[k, rows : rows + 1, :].astype(jnp.float32)
        scaled[:, k * width : (k + 1) * width] = (numbers * gain).astype(jnp.bfloat16)
    factor = row_factor(jnp.sum(total, axis=1, keepdims=True), parts * width)
    pre = dot(scaled[...], both[...]) * factor
    gate = jnp.minimum(pre[:, :hidden], CLAMP_LIMIT)
    up = jnp.clip(pre[:, hidden:], -CLAMP_LIMIT, CLAMP_LIMIT)
    units = (up + 1.0) * (gate * jax.nn.sigmoid(SILU_SHARPNESS * gate))
    out[...] = units.astype(out.dtype)


def down_kernel(hidden, weights, out):
    parts, _, width = hidden.shape
    total = jnp.zeros(out.shape, jnp.float32)
    for k in range(0, parts, 2):
        both = jnp.concatenate([hidden[k], hidden[k + 1]], axis=1)
        side = jnp.concatenate([weights[k, :width, :], weights[k + 1, :width, :]], axis=0)
        total = total + dot(both, side)
    out[...] = total.astype(out.dtype)


def combine_kernel(table, returned, out):
    scale = table[...]
    rows = returned[...]
    total = jnp.zeros(out.shape, jnp.float32)
    for _ in range(3):
        part = scale.astype(jnp.bfloat16)
        total = total + dot(part, rows, ((0,), (0,)))
        scale = scale - part.astype(jnp.float32)
    out[...] = total.astype(out.dtype)


def call(body, outs, *args, scalars=0, **kwargs):
    spaces = [pltpu.SMEM] * scalars + [pltpu.VMEM] * (len(args) - scalars)
    specs = [pl.BlockSpec(memory_space=space) for space in spaces]
    return pl.pallas_call(body, out_shape=outs, in_specs=specs, **kwargs)(*args)


def exchanged(value, axis):
    return lax.all_to_all(value, axis, 0, 0, tiled=True)


def from_partner(value):
    return lax.ppermute(value, "tp_1", [(0, 1), (1, 0)])


def on_device(
    mix_rows,
    mix_gain,
    w_query,
    w_key,
    w_value,
    key_offset,
    w_out,
    out_gain,
    exp_rows,
    exp_gain,
    routes,
    route_weight,
    w_gate,
    w_up,
    w_down,
):
    bf16 = jnp.bfloat16
    shape = jax.ShapeDtypeStruct
    ep_count = lax.axis_size(EP)
    tp_count = lax.axis_size(TP)
    tokens, top = routes.shape
    part = exp_rows.shape[1]
    experts = ep_count * w_gate.shape[0]
    capacity = 4 * tokens * top // (3 * experts)
    slots = experts * capacity
    rows = mix_rows.shape[0]
    head = w_query.shape[0]
    model = mix_rows.shape[1]
    own = jnp.stack([lax.axis_index("ep_0"), lax.axis_index("ep_1")]).astype(jnp.int32)
    core = lax.axis_index("tp_1").astype(jnp.int32)[None]

    along = lax.axis_size("ep_0")
    half = rows // 2
    asked, pairs, outgoing, table = call(
        prepare_kernel,
        (
            shape((along, half, 2 * head), bf16),
            shape((rows, 2 * head), bf16),
            shape((slots, part), bf16),
            shape((slots, tokens), jnp.float32),
        ),
        routes.T,
        route_weight.T,
        exp_rows,
        mix_rows,
        mix_gain,
        w_query,
        w_key,
        w_value,
    )
    arrived = exchanged(outgoing, EP)
    near_pairs = lax.all_gather(pairs, "ep_1", axis=0)
    asked = exchanged(asked, "ep_0")
    gain_rows = jnp.broadcast_to(exp_gain[None], (PAD, part))
    every_row = jnp.concatenate([arrived, gain_rows], axis=0)
    every_row = lax.all_gather(every_row, TP, axis=0)

    columns = call(
        columns_kernel,
        shape((tp_count, w_down.shape[1] + head, model // tp_count), bf16),
        w_down,
        w_out,
    )
    columns = exchanged(columns, TP)

    partial = call(
        attend_kernel,
        shape((along, half + 2 * PAD, 2 * head), bf16),
        own,
        near_pairs,
        asked,
        key_offset,
        scalars=1,
    )
    partial = exchanged(partial, "ep_0")
    attended = call(gather_kernel, shape((half, 2 * head), bf16), partial)

    units = w_gate.shape[2]
    hidden = call(
        expert_kernel,
        shape((slots, units), bf16),
        every_row,
        w_gate,
        w_up,
        scratch_shapes=[
            pltpu.VMEM((slots, model), bf16),
            pltpu.VMEM((model, 2 * units), bf16),
        ],
    )
    every_hidden = lax.all_gather(hidden, TP, axis=0)
    expert_out = call(down_kernel, shape((slots, part), bf16), every_hidden, columns)
    returned = exchanged(expert_out, EP)
    exp_out = call(combine_kernel, shape((tokens, part), bf16), table, returned)

    every_head = lax.all_gather(attended, TP, axis=0)
    own_columns = call(
        mix_columns_kernel,
        shape((tp_count // 2, rows, model // tp_count), bf16),
        every_head,
        columns,
    )
    mine = exchanged(own_columns, "tp_0")
    mix_out = call(
        mix_norm_kernel,
        shape((rows, model), bf16),
        core,
        mine,
        from_partner(mine),
        out_gain,
        scalars=1,
    )
    return (mix_out, exp_out)


def solution(mesh):
    torus = Mesh(mesh.devices.reshape(8, 4, 8, 2), ("ep_0", "ep_1", "tp_0", "tp_1"))
    in_specs = (
        P(EP, None),
        P(),
        P(TP, None),
        P(TP, None),
        P(TP, None),
        P(TP, None),
        P(TP, None),
        P(),
        P(EP, TP),
        P(TP),
        P(EP, None),
        P(EP, None),
        P(EP, None, TP),
        P(EP, None, TP),
        P(EP, TP, None),
    )
    out_specs = (P(EP, None), P(EP, TP))

    def step(*args):
        return on_device(*args)

    step = jax.shard_map(
        step, mesh=torus, in_specs=in_specs, out_specs=out_specs, check_vma=False
    )
    return step
```

```python
import math

import jax
import jax.numpy as jnp
from jax import lax
from jax.experimental import pallas as pl
from jax.experimental.pallas import tpu as pltpu
from jax.sharding import Mesh
from jax.sharding import PartitionSpec as P

EP = ("ep_0", "ep_1")
TP = ("tp_0", "tp_1")

EPSILON = 1e-06
CLAMP_LIMIT = 7.0
SILU_SHARPNESS = 1.702
LOG2E = 1.4426950408889634
PAD = 16


def dot(a, b, dims=((1,), (0,)), precision=None):
    return lax.dot_general(
        a, b, (dims, ((), ())), precision=precision, preferred_element_type=jnp.float32
    )


def row_factor(total, width):
    return lax.rsqrt(total / width + EPSILON)


def prepare_kernel(
    routes, weight, rows, mix_rows, gain, w_query, w_key, w_value, queries, payload, table
):
    top, tokens = routes.shape
    slots = table.shape[0]
    across, _, _ = payload.shape
    positions = mix_rows.shape[0]
    along = slots // (across * PAD)
    capacity = PAD
    slot = lax.broadcasted_iota(jnp.int32, (slots, tokens), 0)
    expert_of = slot // capacity
    place_of = slot - expert_of * capacity
    named = jnp.zeros((slots, tokens), jnp.float32)
    scale = jnp.zeros((slots, tokens), jnp.float32)
    for k in range(top):
        here = routes[k : k + 1, :] == expert_of
        named = jnp.where(here, 1.0, named)
        scale = jnp.where(here, weight[k : k + 1, :], scale)
    earlier = lax.broadcasted_iota(jnp.int32, (tokens, tokens), 0) < lax.broadcasted_iota(
        jnp.int32, (tokens, tokens), 1
    )
    earlier = jnp.where(earlier, 1.0, 0.0).astype(jnp.bfloat16)
    place = dot(named.astype(jnp.bfloat16), earlier)
    mine = (named > 0.0) & (place == place_of.astype(jnp.float32))
    table[...] = jnp.where(mine, scale, 0.0)
    chosen = jnp.where(mine, 1.0, 0.0).astype(jnp.bfloat16)
    outgoing = dot(chosen, rows[...]).astype(payload.dtype)
    for x in range(across):
        for z in range(along):
            at = (z * across + x) * capacity
            to = positions + z * capacity
            payload[x, to : to + capacity, :] = outgoing[at : at + capacity]

    numbers = mix_rows[...].astype(jnp.float32)
    factor = row_factor(jnp.sum(numbers * numbers, axis=1, keepdims=True), numbers.shape[1])
    normed = (numbers * factor * gain[...][None].astype(jnp.float32)).astype(jnp.bfloat16)
    half = positions // 2
    asked = dot(normed, w_query[...], ((1,), (1,))).astype(jnp.bfloat16)
    queries[...] = jnp.concatenate([asked[:half], asked[half:]], axis=1)
    keys = dot(normed, w_key[...], ((1,), (1,)))
    values = dot(normed, w_value[...], ((1,), (1,)))
    pairs = jnp.concatenate([keys, values], axis=1).astype(payload.dtype)
    for x in range(across):
        payload[x, :positions, :] = pairs


def columns_kernel(w_down, w_out, down, out):
    parts, _, width = out.shape
    for k in range(parts):
        at = slice(k * width, (k + 1) * width)
        down[k] = w_down[0, :, at]
        out[k] = w_out[:, at]


def relay_kernel(payload, queries, out):
    across = payload.shape[0]
    along = out.shape[0]
    half = queries.shape[0]
    positions = 2 * half
    own = queries[...]
    for z in range(along):
        at = slice(positions + z * PAD, positions + (z + 1) * PAD)
        for x in range(across):
            out[z, x * PAD : (x + 1) * PAD, :] = payload[x, at, :]
        out[z, across * PAD :, :] = own


def identity(size):
    row = lax.broadcasted_iota(jnp.int32, (size, size), 0)
    return jnp.where(row == lax.broadcasted_iota(jnp.int32, (size, size), 1), 1.0, 0.0)


def attend_kernel(where_ref, payload, asked, offsets, out):
    z, x = where_ref[0], where_ref[1]
    across = payload.shape[0]
    along = asked.shape[0]
    half = asked.shape[1] - across * PAD
    rows = 2 * half
    head = asked.shape[2] // 2
    visible = lax.broadcasted_iota(jnp.int32, (rows, rows), 1) < lax.broadcasted_iota(
        jnp.int32, (rows, rows), 0
    )
    after = jnp.where(visible, -1.0, 0.0).astype(jnp.bfloat16)
    turn = identity(rows).astype(jnp.bfloat16)

    def front(q, j, diagonal):
        pair = payload[j, :rows, :]
        at = pl.multiple_of((z * across + j) * rows, rows)
        s = dot(q, pair[:, :head], ((1,), (1,)))
        s = s * (LOG2E / math.sqrt(head)) + offsets[:, pl.ds(at, rows)] * LOG2E
        soft = jnp.log2(1.0 + jnp.exp2(-jnp.abs(s)))
        take = jnp.minimum(s, 0.0) - soft
        cost = jnp.maximum(s, 0.0) + soft
        if diagonal:
            cost = jnp.where(visible, cost, 0.0)
        inside = dot(cost.astype(jnp.bfloat16), after)
        return take + inside, inside[:, :1] - cost[:, :1], pair[:, head:]

    def back(ahead, state, diagonal):
        later, acc = state
        exponent, total, values = ahead
        w = jnp.exp2(exponent + later)
        if diagonal:
            w = jnp.where(visible, w, 0.0)
        return later + total, acc + dot(w.astype(jnp.bfloat16), values)

    def asked_by(block):
        both = asked[block, across * PAD :, :]
        return jnp.concatenate([both[:, :head], both[:, head:]], axis=0)

    def send(block, state):
        later, acc = state
        acc = acc.astype(out.dtype)
        out[block, :half, :] = jnp.concatenate([acc[:half], acc[half:]], axis=1)
        high = later.astype(jnp.bfloat16)
        low = (later - high.astype(jnp.float32)).astype(jnp.bfloat16)
        wide = (rows, PAD // 2)
        parts = [jnp.broadcast_to(high, wide), jnp.broadcast_to(low, wide)]
        parts = dot(jnp.concatenate(parts, axis=1), turn, ((0,), (0,))).astype(out.dtype)
        out[block, half : half + PAD, :] = parts[:, :half]
        out[block, half + PAD :, :] = parts[:, half:]

    start = (jnp.zeros((rows, 1), jnp.float32), jnp.zeros((rows, head), jnp.float32))

    def nothing(block, carry):
        out[block] = jnp.zeros(out.shape[1:], out.dtype)
        return carry

    def everything(block, carry):
        q = asked_by(block)
        state = start
        ahead = [front(q, across - 1 - i, False) for i in range(across)]
        for one in ahead:
            state = back(one, state, False)
        send(block, state)
        return carry

    lax.fori_loop(0, z, nothing, 0)
    q = asked_by(z)
    state = back(front(q, x, True), start, True)
    state = lax.fori_loop(0, x, lambda i, c: back(front(q, x - 1 - i, False), c, False), state)
    send(z, state)
    lax.fori_loop(z + 1, along, everything, 0)


def gather_kernel(partial, out):
    along, _, width = partial.shape
    half, head = width, width // 2
    rows = 2 * half
    turn = identity(rows).astype(jnp.bfloat16)
    later = jnp.zeros((rows, 1), jnp.float32)
    total = jnp.zeros((rows, head), jnp.float32)
    for g in range(along - 1, -1, -1):
        both = partial[g, :half, :].astype(jnp.float32)
        both = jnp.concatenate([both[:, :head], both[:, head:]], axis=0)
        total = total + jnp.exp2(later) * both
        parts = [partial[g, half : half + PAD, :], partial[g, half + PAD :, :]]
        parts = dot(turn, jnp.concatenate(parts, axis=1), ((1,), (1,)))
        later = later + (parts[:, :1] + parts[:, PAD // 2 : PAD // 2 + 1])
    total = total.astype(out.dtype)
    out[...] = jnp.concatenate([total[:half], total[half:]], axis=1)


def mix_columns_kernel(attended, weights, out):
    parts, half, width = attended.shape
    head = width // 2
    side = jnp.concatenate([weights[k] for k in range(parts)], axis=0)
    top = jnp.concatenate([attended[k][:, :head] for k in range(parts)], axis=1)
    low = jnp.concatenate([attended[k][:, head:] for k in range(parts)], axis=1)
    top = dot(top, side).astype(out.dtype)
    low = dot(low, side).astype(out.dtype)
    for copy in range(out.shape[0]):
        out[copy, :half, :] = top
        out[copy, half:, :] = low


def mix_norm_kernel(core_ref, mine, theirs, gain, out):
    core = core_ref[0]
    groups, rows, width = mine.shape
    total = jnp.zeros((rows, width), jnp.float32)
    for k in range(groups):
        for side in (mine, theirs):
            numbers = side[k].astype(jnp.float32)
            total = total + numbers * numbers
    factor = row_factor(jnp.sum(total, axis=1, keepdims=True), 2 * groups * width)
    scale = gain[...].astype(jnp.float32)[None]
    first = core == 0
    for k in range(groups):
        pair = (mine[k].astype(jnp.float32), theirs[k].astype(jnp.float32))
        for which in range(2):
            at = slice((2 * k + which) * width, (2 * k + which + 1) * width)
            numbers = jnp.where(first, pair[which], pair[1 - which])
            out[:, at] = (numbers * factor * scale[:, at]).astype(out.dtype)


def expert_kernel(arrived, w_gate, w_up, out, scaled, both):
    parts, padded, width = arrived.shape
    rows = padded - PAD
    hidden = w_gate.shape[2]
    both[:, :hidden] = w_gate[0]
    both[:, hidden:] = w_up[0]
    total = jnp.zeros((rows, width), jnp.float32)
    for k in range(parts):
        numbers = arrived[k, :rows, :].astype(jnp.float32)
        total = total + numbers * numbers
        gain = arrived[k, rows : rows + 1, :].astype(jnp.float32)
        scaled[:, k * width : (k + 1) * width] = (numbers * gain).astype(jnp.bfloat16)
    factor = row_factor(jnp.sum(total, axis=1, keepdims=True), parts * width)
    pre = dot(scaled[...], both[...]) * factor
    gate = jnp.minimum(pre[:, :hidden], CLAMP_LIMIT)
    up = jnp.clip(pre[:, hidden:], -CLAMP_LIMIT, CLAMP_LIMIT)
    units = (up + 1.0) * (gate * jax.nn.sigmoid(SILU_SHARPNESS * gate))
    out[...] = units.astype(out.dtype)


def down_kernel(hidden, weights, out):
    parts, _, width = hidden.shape
    total = jnp.zeros(out.shape, jnp.float32)
    for k in range(0, parts, 2):
        both = jnp.concatenate([hidden[k], hidden[k + 1]], axis=1)
        side = jnp.concatenate([weights[k, :width, :], weights[k + 1, :width, :]], axis=0)
        total = total + dot(both, side)
    out[...] = total.astype(out.dtype)


def combine_kernel(table, returned, out):
    scale = table[...]
    rows = returned[...]
    total = jnp.zeros(out.shape, jnp.float32)
    for _ in range(3):
        part = scale.astype(jnp.bfloat16)
        total = total + dot(part, rows, ((0,), (0,)))
        scale = scale - part.astype(jnp.float32)
    out[...] = total.astype(out.dtype)


def call(body, outs, *args, scalars=0, **kwargs):
    spaces = [pltpu.SMEM] * scalars + [pltpu.VMEM] * (len(args) - scalars)
    specs = [pl.BlockSpec(memory_space=space) for space in spaces]
    return pl.pallas_call(body, out_shape=outs, in_specs=specs, **kwargs)(*args)


def exchanged(value, axis):
    return lax.all_to_all(value, axis, 0, 0, tiled=True)


def from_partner(value):
    return lax.ppermute(value, "tp_1", [(0, 1), (1, 0)])


def on_device(
    mix_rows,
    mix_gain,
    w_query,
    w_key,
    w_value,
    key_offset,
    w_out,
    out_gain,
    exp_rows,
    exp_gain,
    routes,
    route_weight,
    w_gate,
    w_up,
    w_down,
):
    bf16 = jnp.bfloat16
    shape = jax.ShapeDtypeStruct
    ep_count = lax.axis_size(EP)
    tp_count = lax.axis_size(TP)
    tokens, top = routes.shape
    part = exp_rows.shape[1]
    experts = ep_count * w_gate.shape[0]
    capacity = 4 * tokens * top // (3 * experts)
    slots = experts * capacity
    rows = mix_rows.shape[0]
    head = w_query.shape[0]
    model = mix_rows.shape[1]
    own = jnp.stack([lax.axis_index("ep_0"), lax.axis_index("ep_1")]).astype(jnp.int32)
    core = lax.axis_index("tp_1").astype(jnp.int32)[None]

    across = lax.axis_size("ep_1")
    along = lax.axis_size("ep_0")
    half = rows // 2
    queries, payload, table = call(
        prepare_kernel,
        (
            shape((half, 2 * head), bf16),
            shape((across, rows + along * capacity, part), bf16),
            shape((slots, tokens), jnp.float32),
        ),
        routes.T,
        route_weight.T,
        exp_rows,
        mix_rows,
        mix_gain,
        w_query,
        w_key,
        w_value,
    )
    payload = exchanged(payload, "ep_1")
    asked = call(
        relay_kernel, shape((along, across * capacity + half, part), bf16), payload, queries
    )
    asked = exchanged(asked, "ep_0")
    arrived = asked[:, : across * capacity].reshape(slots, part)
    gain_rows = jnp.broadcast_to(exp_gain[None], (PAD, part))
    every_row = jnp.concatenate([arrived, gain_rows], axis=0)
    every_row = lax.all_gather(every_row, TP, axis=0)

    columns = (tp_count, w_out.shape[0], model // tp_count)
    down_columns, out_columns = call(
        columns_kernel,
        (shape((tp_count, w_down.shape[1], columns[2]), bf16), shape(columns, bf16)),
        w_down,
        w_out,
    )
    out_columns = exchanged(out_columns, TP)
    down_columns = exchanged(down_columns, TP)

    partial = call(
        attend_kernel,
        shape((along, half + 2 * PAD, 2 * head), bf16),
        own,
        payload,
        asked,
        key_offset,
        scalars=1,
    )
    partial = exchanged(partial, "ep_0")
    attended = call(gather_kernel, shape((half, 2 * head), bf16), partial)

    units = w_gate.shape[2]
    hidden = call(
        expert_kernel,
        shape((slots, units), bf16),
        every_row,
        w_gate,
        w_up,
        scratch_shapes=[
            pltpu.VMEM((slots, model), bf16),
            pltpu.VMEM((model, 2 * units), bf16),
        ],
    )
    every_hidden = lax.all_gather(hidden, TP, axis=0)
    expert_out = call(down_kernel, shape((slots, part), bf16), every_hidden, down_columns)
    returned = exchanged(expert_out, EP)
    exp_out = call(combine_kernel, shape((tokens, part), bf16), table, returned)

    every_head = lax.all_gather(attended, TP, axis=0)
    own_columns = call(
        mix_columns_kernel,
        shape((tp_count // 2, rows, model // tp_count), bf16),
        every_head,
        out_columns,
    )
    mine = exchanged(own_columns, "tp_0")
    mix_out = call(
        mix_norm_kernel,
        shape((rows, model), bf16),
        core,
        mine,
        from_partner(mine),
        out_gain,
        scalars=1,
    )
    return (mix_out, exp_out)


def solution(mesh):
    torus = Mesh(mesh.devices.reshape(8, 4, 8, 2), ("ep_0", "ep_1", "tp_0", "tp_1"))
    in_specs = (
        P(EP, None),
        P(),
        P(TP, None),
        P(TP, None),
        P(TP, None),
        P(TP, None),
        P(TP, None),
        P(),
        P(EP, TP),
        P(TP),
        P(EP, None),
        P(EP, None),
        P(EP, None, TP),
        P(EP, None, TP),
        P(EP, TP, None),
    )
    out_specs = (P(EP, None), P(EP, TP))

    def step(*args):
        return on_device(*args)

    step = jax.shard_map(
        step, mesh=torus, in_specs=in_specs, out_specs=out_specs, check_vma=False
    )
    return step
```

```python
import math

import jax
import jax.numpy as jnp
from jax import lax
from jax.experimental import pallas as pl
from jax.experimental.pallas import tpu as pltpu
from jax.sharding import Mesh
from jax.sharding import PartitionSpec as P

EP = ("ep_0", "ep_1")
TP = ("tp_0", "tp_1")

EPSILON = 1e-06
CLAMP_LIMIT = 7.0
SILU_SHARPNESS = 1.702
LOG2E = 1.4426950408889634
PAD = 16


def dot(a, b, dims=((1,), (0,)), precision=None):
    return lax.dot_general(
        a, b, (dims, ((), ())), precision=precision, preferred_element_type=jnp.float32
    )


def row_factor(total, width):
    return lax.rsqrt(total / width + EPSILON)


def prepare_kernel(
    routes,
    weight,
    rows,
    mix_rows,
    gain,
    w_query,
    w_key,
    w_value,
    queries,
    payload,
    table,
    every,
):
    top, tokens = routes.shape
    slots = table.shape[0]
    across, _, _ = payload.shape
    positions = mix_rows.shape[0]
    along = slots // (across * PAD)
    capacity = PAD
    slot = lax.broadcasted_iota(jnp.int32, (slots, tokens), 0)
    expert_of = slot // capacity
    place_of = slot - expert_of * capacity
    named = jnp.zeros((slots, tokens), jnp.float32)
    scale = jnp.zeros((slots, tokens), jnp.float32)
    for k in range(top):
        here = routes[k : k + 1, :] == expert_of
        named = jnp.where(here, 1.0, named)
        scale = jnp.where(here, weight[k : k + 1, :], scale)
    earlier = lax.broadcasted_iota(jnp.int32, (tokens, tokens), 0) < lax.broadcasted_iota(
        jnp.int32, (tokens, tokens), 1
    )
    earlier = jnp.where(earlier, 1.0, 0.0).astype(jnp.bfloat16)
    place = dot(named.astype(jnp.bfloat16), earlier)
    mine = (named > 0.0) & (place == place_of.astype(jnp.float32))
    table[...] = jnp.where(mine, scale, 0.0)
    chosen = jnp.where(mine, 1.0, 0.0).astype(jnp.bfloat16)
    outgoing = dot(chosen, rows[...]).astype(payload.dtype)
    for x in range(across):
        for z in range(along):
            at = (z * across + x) * capacity
            to = positions + z * capacity
            payload[x, to : to + capacity, :] = outgoing[at : at + capacity]

    numbers = mix_rows[...].astype(jnp.float32)
    factor = row_factor(jnp.sum(numbers * numbers, axis=1, keepdims=True), numbers.shape[1])
    normed = (numbers * factor * gain[...][None].astype(jnp.float32)).astype(jnp.bfloat16)
    half = positions // 2
    head = w_query.shape[0]
    every[:head, :] = w_query[...]
    every[head : 2 * head, :] = w_key[...]
    every[2 * head :, :] = w_value[...]
    both = dot(normed, every[...], ((1,), (1,))).astype(jnp.bfloat16)
    asked = both[:, :head]
    queries[...] = jnp.concatenate([asked[:half], asked[half:]], axis=1)
    pairs = both[:, head:]
    for x in range(across):
        payload[x, :positions, :] = pairs


def columns_kernel(w_down, w_out, table, out, turned):
    parts, _, width = out.shape
    scale = table[...]
    slots, _ = scale.shape
    turn = identity(slots).astype(jnp.bfloat16)
    for k in range(turned.shape[0]):
        piece = scale.astype(jnp.bfloat16)
        scale = scale - piece.astype(jnp.float32)
        turned[k] = dot(piece, turn, ((0,), (0,))).astype(jnp.bfloat16)
    hidden = w_down.shape[1]
    for k in range(parts):
        at = slice(k * width, (k + 1) * width)
        out[k, :hidden, :] = w_down[0, :, at]
        out[k, hidden:, :] = w_out[:, at]


def relay_kernel(payload, queries, out):
    across = payload.shape[0]
    along = out.shape[0]
    half = queries.shape[0]
    positions = 2 * half
    own = queries[...]
    for z in range(along):
        at = slice(positions + z * PAD, positions + (z + 1) * PAD)
        for x in range(across):
            out[z, x * PAD : (x + 1) * PAD, :] = payload[x, at, :]
        out[z, across * PAD :, :] = own


def identity(size):
    row = lax.broadcasted_iota(jnp.int32, (size, size), 0)
    return jnp.where(row == lax.broadcasted_iota(jnp.int32, (size, size), 1), 1.0, 0.0)


def attend_kernel(where_ref, payload, asked, offsets, out):
    z, x = where_ref[0], where_ref[1]
    across = payload.shape[0]
    along = asked.shape[0]
    half = asked.shape[1] - across * PAD
    rows = 2 * half
    head = asked.shape[2] // 2
    visible = lax.broadcasted_iota(jnp.int32, (rows, rows), 1) < lax.broadcasted_iota(
        jnp.int32, (rows, rows), 0
    )
    after = jnp.where(visible, -1.0, 0.0).astype(jnp.bfloat16)
    turn = identity(rows).astype(jnp.bfloat16)

    def front(q, j, diagonal):
        pair = payload[j, :rows, :]
        at = pl.multiple_of((z * across + j) * rows, rows)
        s = dot(q, pair[:, :head], ((1,), (1,)))
        s = s * (LOG2E / math.sqrt(head)) + offsets[:, pl.ds(at, rows)] * LOG2E
        soft = jnp.log2(1.0 + jnp.exp2(-jnp.abs(s)))
        take = jnp.minimum(s, 0.0) - soft
        cost = jnp.maximum(s, 0.0) + soft
        if diagonal:
            cost = jnp.where(visible, cost, 0.0)
        inside = dot(cost.astype(jnp.bfloat16), after)
        return take + inside, inside[:, :1] - cost[:, :1], pair[:, head:]

    def back(ahead, state, diagonal):
        later, acc = state
        exponent, total, values = ahead
        w = jnp.exp2(exponent + later)
        if diagonal:
            w = jnp.where(visible, w, 0.0)
        return later + total, acc + dot(w.astype(jnp.bfloat16), values)

    def asked_by(block):
        both = asked[block, across * PAD :, :]
        return jnp.concatenate([both[:, :head], both[:, head:]], axis=0)

    def send(block, state):
        later, acc = state
        acc = acc.astype(out.dtype)
        out[block, :half, :] = jnp.concatenate([acc[:half], acc[half:]], axis=1)
        high = later.astype(jnp.bfloat16)
        low = (later - high.astype(jnp.float32)).astype(jnp.bfloat16)
        wide = (rows, PAD // 2)
        parts = [jnp.broadcast_to(high, wide), jnp.broadcast_to(low, wide)]
        parts = dot(jnp.concatenate(parts, axis=1), turn, ((0,), (0,))).astype(out.dtype)
        out[block, half : half + PAD, :] = parts[:, :half]
        out[block, half + PAD :, :] = parts[:, half:]

    start = (jnp.zeros((rows, 1), jnp.float32), jnp.zeros((rows, head), jnp.float32))

    def nothing(block, carry):
        out[block] = jnp.zeros(out.shape[1:], out.dtype)
        return carry

    def everything(block, carry):
        q = asked_by(block)
        state = start
        ahead = [front(q, across - 1 - i, False) for i in range(across)]
        for one in ahead:
            state = back(one, state, False)
        send(block, state)
        return carry

    lax.fori_loop(0, z, nothing, 0)
    q = asked_by(z)
    state = back(front(q, x, True), start, True)
    state = lax.fori_loop(0, x, lambda i, c: back(front(q, x - 1 - i, False), c, False), state)
    send(z, state)
    lax.fori_loop(z + 1, along, everything, 0)


def gather_kernel(partial, out):
    along, _, width = partial.shape
    half, head = width, width // 2
    rows = 2 * half
    turn = identity(rows).astype(jnp.bfloat16)
    later = jnp.zeros((rows, 1), jnp.float32)
    total = jnp.zeros((rows, head), jnp.float32)
    for g in range(along - 1, -1, -1):
        both = partial[g, :half, :].astype(jnp.float32)
        both = jnp.concatenate([both[:, :head], both[:, head:]], axis=0)
        total = total + jnp.exp2(later) * both
        parts = [partial[g, half : half + PAD, :], partial[g, half + PAD :, :]]
        parts = dot(turn, jnp.concatenate(parts, axis=1), ((1,), (1,)))
        later = later + (parts[:, :1] + parts[:, PAD // 2 : PAD // 2 + 1])
    total = total.astype(out.dtype)
    out[...] = jnp.concatenate([total[:half], total[half:]], axis=1)


def mix_columns_kernel(attended, weights, out):
    parts, half, width = attended.shape
    head = width // 2
    skip = weights.shape[1] - head
    side = jnp.concatenate([weights[k, skip:, :] for k in range(parts)], axis=0)
    top = jnp.concatenate([attended[k][:, :head] for k in range(parts)], axis=1)
    low = jnp.concatenate([attended[k][:, head:] for k in range(parts)], axis=1)
    top = dot(top, side).astype(out.dtype)
    low = dot(low, side).astype(out.dtype)
    for copy in range(out.shape[0]):
        out[copy, :half, :] = top
        out[copy, half:, :] = low


def mix_norm_kernel(core_ref, mine, theirs, gain, out):
    core = core_ref[0]
    groups, rows, width = mine.shape
    total = jnp.zeros((rows, width), jnp.float32)
    for k in range(groups):
        for side in (mine, theirs):
            numbers = side[k].astype(jnp.float32)
            total = total + numbers * numbers
    factor = row_factor(jnp.sum(total, axis=1, keepdims=True), 2 * groups * width)
    scale = gain[...].astype(jnp.float32)[None]
    first = core == 0
    for k in range(groups):
        pair = (mine[k].astype(jnp.float32), theirs[k].astype(jnp.float32))
        for which in range(2):
            at = slice((2 * k + which) * width, (2 * k + which + 1) * width)
            numbers = jnp.where(first, pair[which], pair[1 - which])
            out[:, at] = (numbers * factor * scale[:, at]).astype(out.dtype)


def expert_kernel(arrived, w_gate, w_up, out, scaled, both):
    parts, padded, width = arrived.shape
    rows = padded - PAD
    hidden = w_gate.shape[2]
    both[:, :hidden] = w_gate[0]
    both[:, hidden:] = w_up[0]
    total = jnp.zeros((rows, width), jnp.float32)
    for k in range(parts):
        numbers = arrived[k, :rows, :].astype(jnp.float32)
        total = total + numbers * numbers
        gain = arrived[k, rows : rows + 1, :].astype(jnp.float32)
        scaled[:, k * width : (k + 1) * width] = (numbers * gain).astype(jnp.bfloat16)
    factor = row_factor(jnp.sum(total, axis=1, keepdims=True), parts * width)
    pre = dot(scaled[...], both[...]) * factor
    gate = jnp.minimum(pre[:, :hidden], CLAMP_LIMIT)
    up = jnp.clip(pre[:, hidden:], -CLAMP_LIMIT, CLAMP_LIMIT)
    units = (up + 1.0) * (gate * jax.nn.sigmoid(SILU_SHARPNESS * gate))
    out[...] = units.astype(out.dtype)


def down_kernel(hidden, weights, out):
    parts, _, width = hidden.shape
    total = jnp.zeros(out.shape, jnp.float32)
    for k in range(0, parts, 2):
        both = jnp.concatenate([hidden[k], hidden[k + 1]], axis=1)
        side = jnp.concatenate([weights[k, :width, :], weights[k + 1, :width, :]], axis=0)
        total = total + dot(both, side)
    out[...] = total.astype(out.dtype)


def combine_kernel(table, returned, out):
    rows = returned[...]
    total = dot(table[0], rows) + dot(table[1], rows)
    out[...] = total.astype(out.dtype)


def call(body, outs, *args, scalars=0, **kwargs):
    spaces = [pltpu.SMEM] * scalars + [pltpu.VMEM] * (len(args) - scalars)
    specs = [pl.BlockSpec(memory_space=space) for space in spaces]
    return pl.pallas_call(body, out_shape=outs, in_specs=specs, **kwargs)(*args)


def exchanged(value, axis):
    return lax.all_to_all(value, axis, 0, 0, tiled=True)


def from_partner(value):
    return lax.ppermute(value, "tp_1", [(0, 1), (1, 0)])


def on_device(
    mix_rows,
    mix_gain,
    w_query,
    w_key,
    w_value,
    key_offset,
    w_out,
    out_gain,
    exp_rows,
    exp_gain,
    routes,
    route_weight,
    w_gate,
    w_up,
    w_down,
):
    bf16 = jnp.bfloat16
    shape = jax.ShapeDtypeStruct
    ep_count = lax.axis_size(EP)
    tp_count = lax.axis_size(TP)
    tokens, top = routes.shape
    part = exp_rows.shape[1]
    experts = ep_count * w_gate.shape[0]
    capacity = 4 * tokens * top // (3 * experts)
    slots = experts * capacity
    rows = mix_rows.shape[0]
    head = w_query.shape[0]
    model = mix_rows.shape[1]
    own = jnp.stack([lax.axis_index("ep_0"), lax.axis_index("ep_1")]).astype(jnp.int32)
    core = lax.axis_index("tp_1").astype(jnp.int32)[None]

    across = lax.axis_size("ep_1")
    along = lax.axis_size("ep_0")
    half = rows // 2
    queries, payload, table = call(
        prepare_kernel,
        (
            shape((half, 2 * head), bf16),
            shape((across, rows + along * capacity, part), bf16),
            shape((slots, tokens), jnp.float32),
        ),
        routes.T,
        route_weight.T,
        exp_rows,
        mix_rows,
        mix_gain,
        w_query,
        w_key,
        w_value,
        scratch_shapes=[pltpu.VMEM((3 * head, model), bf16)],
    )
    payload = exchanged(payload, "ep_1")
    asked = call(
        relay_kernel, shape((along, across * capacity + half, part), bf16), payload, queries
    )
    asked = exchanged(asked, "ep_0")
    arrived = asked[:, : across * capacity].reshape(slots, part)
    gain_rows = jnp.broadcast_to(exp_gain[None], (PAD, part))
    every_row = jnp.concatenate([arrived, gain_rows], axis=0)
    every_row = lax.all_gather(every_row, TP, axis=0)

    columns, turned = call(
        columns_kernel,
        (
            shape((tp_count, w_down.shape[1] + head, model // tp_count), bf16),
            shape((2, tokens, slots), bf16),
        ),
        w_down,
        w_out,
        table,
    )
    columns = exchanged(columns, TP)

    partial = call(
        attend_kernel,
        shape((along, half + 2 * PAD, 2 * head), bf16),
        own,
        payload,
        asked,
        key_offset,
        scalars=1,
    )
    partial = exchanged(partial, "ep_0")
    attended = call(gather_kernel, shape((half, 2 * head), bf16), partial)

    units = w_gate.shape[2]
    hidden = call(
        expert_kernel,
        shape((slots, units), bf16),
        every_row,
        w_gate,
        w_up,
        scratch_shapes=[
            pltpu.VMEM((slots, model), bf16),
            pltpu.VMEM((model, 2 * units), bf16),
        ],
    )
    every_hidden = lax.all_gather(hidden, TP, axis=0)
    expert_out = call(down_kernel, shape((slots, part), bf16), every_hidden, columns)
    returned = exchanged(expert_out, EP)
    exp_out = call(combine_kernel, shape((tokens, part), bf16), turned, returned)

    every_head = lax.all_gather(attended, TP, axis=0)
    own_columns = call(
        mix_columns_kernel,
        shape((tp_count // 2, rows, model // tp_count), bf16),
        every_head,
        columns,
    )
    mine = exchanged(own_columns, "tp_0")
    mix_out = call(
        mix_norm_kernel,
        shape((rows, model), bf16),
        core,
        mine,
        from_partner(mine),
        out_gain,
        scalars=1,
    )
    return (mix_out, exp_out)


def solution(mesh):
    torus = Mesh(mesh.devices.reshape(8, 4, 8, 2), ("ep_0", "ep_1", "tp_0", "tp_1"))
    in_specs = (
        P(EP, None),
        P(),
        P(TP, None),
        P(TP, None),
        P(TP, None),
        P(TP, None),
        P(TP, None),
        P(),
        P(EP, TP),
        P(TP),
        P(EP, None),
        P(EP, None),
        P(EP, None, TP),
        P(EP, None, TP),
        P(EP, TP, None),
    )
    out_specs = (P(EP, None), P(EP, TP))

    def step(*args):
        return on_device(*args)

    step = jax.shard_map(
        step, mesh=torus, in_specs=in_specs, out_specs=out_specs, check_vma=False
    )
    return step
```

```python
import math

import jax
import jax.numpy as jnp
from jax import lax
from jax.experimental import pallas as pl
from jax.experimental.pallas import tpu as pltpu
from jax.sharding import Mesh
from jax.sharding import PartitionSpec as P

EP = ("ep_0", "ep_1")
TP = ("tp_0", "tp_1")

EPSILON = 1e-06
CLAMP_LIMIT = 7.0
SILU_SHARPNESS = 1.702
LOG2E = 1.4426950408889634
PAD = 16


def dot(a, b, dims=((1,), (0,)), precision=None):
    return lax.dot_general(
        a, b, (dims, ((), ())), precision=precision, preferred_element_type=jnp.float32
    )


def row_factor(total, width):
    return lax.rsqrt(total / width + EPSILON)


def prepare_kernel(
    routes,
    weight,
    rows,
    mix_rows,
    gain,
    w_query,
    w_key,
    w_value,
    queries,
    payload,
    table,
    every,
):
    top, tokens = routes.shape
    slots = table.shape[0]
    across, _, _ = payload.shape
    positions = mix_rows.shape[0]
    along = slots // (across * PAD)
    capacity = PAD
    slot = lax.broadcasted_iota(jnp.int32, (slots, tokens), 0)
    expert_of = slot // capacity
    place_of = slot - expert_of * capacity
    named = jnp.zeros((slots, tokens), jnp.float32)
    scale = jnp.zeros((slots, tokens), jnp.float32)
    for k in range(top):
        here = routes[k : k + 1, :] == expert_of
        named = jnp.where(here, 1.0, named)
        scale = jnp.where(here, weight[k : k + 1, :], scale)
    earlier = lax.broadcasted_iota(jnp.int32, (tokens, tokens), 0) < lax.broadcasted_iota(
        jnp.int32, (tokens, tokens), 1
    )
    earlier = jnp.where(earlier, 1.0, 0.0).astype(jnp.bfloat16)
    place = dot(named.astype(jnp.bfloat16), earlier)
    mine = (named > 0.0) & (place == place_of.astype(jnp.float32))
    table[...] = jnp.where(mine, scale, 0.0)
    chosen = jnp.where(mine, 1.0, 0.0).astype(jnp.bfloat16)
    outgoing = dot(chosen, rows[...]).astype(payload.dtype)
    for x in range(across):
        for z in range(along):
            at = (z * across + x) * capacity
            to = positions + z * capacity
            payload[x, to : to + capacity, :] = outgoing[at : at + capacity]

    numbers = mix_rows[...].astype(jnp.float32)
    factor = row_factor(jnp.sum(numbers * numbers, axis=1, keepdims=True), numbers.shape[1])
    normed = (numbers * factor * gain[...][None].astype(jnp.float32)).astype(jnp.bfloat16)
    half = positions // 2
    head = w_query.shape[0]
    every[:head, :] = w_query[...]
    every[head : 2 * head, :] = w_key[...]
    every[2 * head :, :] = w_value[...]
    both = dot(normed, every[...], ((1,), (1,))).astype(jnp.bfloat16)
    asked = both[:, :head]
    queries[...] = jnp.concatenate([asked[:half], asked[half:]], axis=1)
    pairs = both[:, head:]
    for x in range(across):
        payload[x, :positions, :] = pairs


def columns_kernel(w_down, w_out, table, out, turned):
    parts, _, width = out.shape
    scale = table[...]
    slots, _ = scale.shape
    turn = identity(slots).astype(jnp.bfloat16)
    for k in range(turned.shape[0]):
        piece = scale.astype(jnp.bfloat16)
        scale = scale - piece.astype(jnp.float32)
        turned[k] = dot(piece, turn, ((0,), (0,))).astype(jnp.bfloat16)
    hidden = w_down.shape[1]
    for k in range(parts):
        at = slice(k * width, (k + 1) * width)
        out[k, :hidden, :] = w_down[0, :, at]
        out[k, hidden:, :] = w_out[:, at]


def relay_kernel(payload, queries, out):
    across = payload.shape[0]
    along = out.shape[0]
    half = queries.shape[0]
    positions = 2 * half
    own = queries[...]
    for z in range(along):
        at = slice(positions + z * PAD, positions + (z + 1) * PAD)
        for x in range(across):
            out[z, x * PAD : (x + 1) * PAD, :] = payload[x, at, :]
        out[z, across * PAD :, :] = own


def identity(size):
    row = lax.broadcasted_iota(jnp.int32, (size, size), 0)
    return jnp.where(row == lax.broadcasted_iota(jnp.int32, (size, size), 1), 1.0, 0.0)


def attend_kernel(z_ref, x_ref, payload, asked, offsets, out):
    z, x = z_ref[0], x_ref[0]
    across = payload.shape[0]
    along = asked.shape[0]
    half = asked.shape[1] - across * PAD
    rows = 2 * half
    head = asked.shape[2] // 2
    visible = lax.broadcasted_iota(jnp.int32, (rows, rows), 1) < lax.broadcasted_iota(
        jnp.int32, (rows, rows), 0
    )
    after = jnp.where(visible, -1.0, 0.0).astype(jnp.bfloat16)
    turn = identity(rows).astype(jnp.bfloat16)

    def front(q, j, diagonal):
        pair = payload[j, :rows, :]
        at = pl.multiple_of((z * across + j) * rows, rows)
        s = dot(q, pair[:, :head], ((1,), (1,)))
        s = s * (LOG2E / math.sqrt(head)) + offsets[:, pl.ds(at, rows)] * LOG2E
        soft = jnp.log2(1.0 + jnp.exp2(-jnp.abs(s)))
        take = jnp.minimum(s, 0.0) - soft
        cost = jnp.maximum(s, 0.0) + soft
        if diagonal:
            cost = jnp.where(visible, cost, 0.0)
        inside = dot(cost.astype(jnp.bfloat16), after)
        return take + inside, inside[:, :1] - cost[:, :1], pair[:, head:]

    def back(ahead, state, diagonal):
        later, acc = state
        exponent, total, values = ahead
        w = jnp.exp2(exponent + later)
        if diagonal:
            w = jnp.where(visible, w, 0.0)
        return later + total, acc + dot(w.astype(jnp.bfloat16), values)

    def asked_by(block):
        both = asked[block, across * PAD :, :]
        return jnp.concatenate([both[:, :head], both[:, head:]], axis=0)

    def send(block, state):
        later, acc = state
        acc = acc.astype(out.dtype)
        out[block, :half, :] = jnp.concatenate([acc[:half], acc[half:]], axis=1)
        high = later.astype(jnp.bfloat16)
        low = (later - high.astype(jnp.float32)).astype(jnp.bfloat16)
        wide = (rows, PAD // 2)
        parts = [jnp.broadcast_to(high, wide), jnp.broadcast_to(low, wide)]
        parts = dot(jnp.concatenate(parts, axis=1), turn, ((0,), (0,))).astype(out.dtype)
        out[block, half : half + PAD, :] = parts[:, :half]
        out[block, half + PAD :, :] = parts[:, half:]

    start = (jnp.zeros((rows, 1), jnp.float32), jnp.zeros((rows, head), jnp.float32))

    def nothing(block, carry):
        out[block] = jnp.zeros(out.shape[1:], out.dtype)
        return carry

    def everything(blocks, carry):
        asked_now = [asked_by(block) for block in blocks]
        ahead = [[front(q, across - 1 - i, False) for i in range(across)] for q in asked_now]
        for block, terms in zip(blocks, ahead):
            state = start
            for one in terms:
                state = back(one, state, False)
            send(block, state)
        return carry

    lax.fori_loop(0, z, nothing, 0)
    q = asked_by(z)
    state = back(front(q, x, True), start, True)
    state = lax.fori_loop(0, x, lambda i, c: back(front(q, x - 1 - i, False), c, False), state)
    send(z, state)
    rest = along - 1 - z
    lax.fori_loop(0, rest % 2, lambda i, c: everything([along - 1], c), 0)
    lax.fori_loop(
        0, rest // 2, lambda i, c: everything([z + 1 + 2 * i, z + 2 + 2 * i], c), 0
    )


def gather_kernel(partial, out):
    along, _, width = partial.shape
    half, head = width, width // 2
    rows = 2 * half
    turn = identity(rows).astype(jnp.bfloat16)
    later = jnp.zeros((rows, 1), jnp.float32)
    total = jnp.zeros((rows, head), jnp.float32)
    for g in range(along - 1, -1, -1):
        both = partial[g, :half, :].astype(jnp.float32)
        both = jnp.concatenate([both[:, :head], both[:, head:]], axis=0)
        total = total + jnp.exp2(later) * both
        parts = [partial[g, half : half + PAD, :], partial[g, half + PAD :, :]]
        parts = dot(turn, jnp.concatenate(parts, axis=1), ((1,), (1,)))
        later = later + (parts[:, :1] + parts[:, PAD // 2 : PAD // 2 + 1])
    total = total.astype(out.dtype)
    out[...] = jnp.concatenate([total[:half], total[half:]], axis=1)


def mix_columns_kernel(attended, weights, out):
    parts, half, width = attended.shape
    head = width // 2
    skip = weights.shape[1] - head
    side = jnp.concatenate([weights[k, skip:, :] for k in range(parts)], axis=0)
    top = jnp.concatenate([attended[k][:, :head] for k in range(parts)], axis=1)
    low = jnp.concatenate([attended[k][:, head:] for k in range(parts)], axis=1)
    top = dot(top, side).astype(out.dtype)
    low = dot(low, side).astype(out.dtype)
    for copy in range(out.shape[0]):
        out[copy, :half, :] = top
        out[copy, half:, :] = low


def mix_norm_kernel(core_ref, mine, theirs, gain, out):
    core = core_ref[0]
    groups, rows, width = mine.shape
    total = jnp.zeros((rows, width), jnp.float32)
    for k in range(groups):
        for side in (mine, theirs):
            numbers = side[k].astype(jnp.float32)
            total = total + numbers * numbers
    factor = row_factor(jnp.sum(total, axis=1, keepdims=True), 2 * groups * width)
    scale = gain[...].astype(jnp.float32)[None]
    first = core == 0
    for k in range(groups):
        pair = (mine[k].astype(jnp.float32), theirs[k].astype(jnp.float32))
        for which in range(2):
            at = slice((2 * k + which) * width, (2 * k + which + 1) * width)
            numbers = jnp.where(first, pair[which], pair[1 - which])
            out[:, at] = (numbers * factor * scale[:, at]).astype(out.dtype)


def expert_kernel(arrived, w_gate, w_up, out, scaled, both):
    parts, padded, width = arrived.shape
    rows = padded - PAD
    hidden = w_gate.shape[2]
    both[:, :hidden] = w_gate[0]
    both[:, hidden:] = w_up[0]
    total = jnp.zeros((rows, width), jnp.float32)
    for k in range(parts):
        numbers = arrived[k, :rows, :].astype(jnp.float32)
        total = total + numbers * numbers
        gain = arrived[k, rows : rows + 1, :].astype(jnp.float32)
        scaled[:, k * width : (k + 1) * width] = (numbers * gain).astype(jnp.bfloat16)
    factor = row_factor(jnp.sum(total, axis=1, keepdims=True), parts * width)
    pre = dot(scaled[...], both[...]) * factor
    gate = jnp.minimum(pre[:, :hidden], CLAMP_LIMIT)
    up = jnp.clip(pre[:, hidden:], -CLAMP_LIMIT, CLAMP_LIMIT)
    units = (up + 1.0) * (gate * jax.nn.sigmoid(SILU_SHARPNESS * gate))
    out[...] = units.astype(out.dtype)


def down_kernel(hidden, weights, out):
    parts, _, width = hidden.shape
    total = jnp.zeros(out.shape, jnp.float32)
    for k in range(0, parts, 2):
        both = jnp.concatenate([hidden[k], hidden[k + 1]], axis=1)
        side = jnp.concatenate([weights[k, :width, :], weights[k + 1, :width, :]], axis=0)
        total = total + dot(both, side)
    out[...] = total.astype(out.dtype)


def call(body, outs, *args, scalars=0, **kwargs):
    spaces = [pltpu.SMEM] * scalars + [pltpu.VMEM] * (len(args) - scalars)
    specs = [pl.BlockSpec(memory_space=space) for space in spaces]
    return pl.pallas_call(body, out_shape=outs, in_specs=specs, **kwargs)(*args)


def exchanged(value, axis):
    return lax.all_to_all(value, axis, 0, 0, tiled=True)


def from_partner(value):
    return lax.ppermute(value, "tp_1", [(0, 1), (1, 0)])


def on_device(
    mix_rows,
    mix_gain,
    w_query,
    w_key,
    w_value,
    key_offset,
    w_out,
    out_gain,
    exp_rows,
    exp_gain,
    routes,
    route_weight,
    w_gate,
    w_up,
    w_down,
):
    bf16 = jnp.bfloat16
    shape = jax.ShapeDtypeStruct
    ep_count = lax.axis_size(EP)
    tp_count = lax.axis_size(TP)
    tokens, top = routes.shape
    part = exp_rows.shape[1]
    experts = ep_count * w_gate.shape[0]
    capacity = 4 * tokens * top // (3 * experts)
    slots = experts * capacity
    rows = mix_rows.shape[0]
    head = w_query.shape[0]
    model = mix_rows.shape[1]
    core = lax.axis_index("tp_1").astype(jnp.int32)[None]

    across = lax.axis_size("ep_1")
    along = lax.axis_size("ep_0")
    half = rows // 2
    queries, payload, table = call(
        prepare_kernel,
        (
            shape((half, 2 * head), bf16),
            shape((across, rows + along * capacity, part), bf16),
            shape((slots, tokens), jnp.float32),
        ),
        routes.T,
        route_weight.T,
        exp_rows,
        mix_rows,
        mix_gain,
        w_query,
        w_key,
        w_value,
        scratch_shapes=[pltpu.VMEM((3 * head, model), bf16)],
    )
    payload = exchanged(payload, "ep_1")
    asked = call(
        relay_kernel, shape((along, across * capacity + half, part), bf16), payload, queries
    )
    asked = exchanged(asked, "ep_0")
    arrived = asked[:, : across * capacity].reshape(slots, part)
    gain_rows = jnp.broadcast_to(exp_gain[None], (PAD, part))
    every_row = jnp.concatenate([arrived, gain_rows], axis=0)
    every_row = lax.all_gather(every_row, TP, axis=0)

    columns, turned = call(
        columns_kernel,
        (
            shape((tp_count, w_down.shape[1] + head, model // tp_count), bf16),
            shape((2, tokens, slots), bf16),
        ),
        w_down,
        w_out,
        table,
    )
    columns = exchanged(columns, TP)

    partial = call(
        attend_kernel,
        shape((along, half + 2 * PAD, 2 * head), bf16),
        lax.axis_index("ep_0").astype(jnp.int32)[None],
        lax.axis_index("ep_1").astype(jnp.int32)[None],
        payload,
        asked,
        key_offset,
        scalars=2,
    )
    partial = exchanged(partial, "ep_0")
    attended = call(gather_kernel, shape((half, 2 * head), bf16), partial)

    units = w_gate.shape[2]
    hidden = call(
        expert_kernel,
        shape((slots, units), bf16),
        every_row,
        w_gate,
        w_up,
        scratch_shapes=[
            pltpu.VMEM((slots, model), bf16),
            pltpu.VMEM((model, 2 * units), bf16),
        ],
    )
    every_hidden = lax.all_gather(hidden, TP, axis=0)
    expert_out = call(down_kernel, shape((slots, part), bf16), every_hidden, columns)
    returned = exchanged(expert_out, EP)
    returned = returned.reshape(slots, part)
    combined = dot(turned.reshape(2 * tokens, slots), returned).reshape(2, tokens, part)
    exp_out = (combined[0] + combined[1]).astype(bf16)

    every_head = lax.all_gather(attended, TP, axis=0)
    own_columns = call(
        mix_columns_kernel,
        shape((tp_count // 2, rows, model // tp_count), bf16),
        every_head,
        columns,
    )
    mine = exchanged(own_columns, "tp_0")
    mix_out = call(
        mix_norm_kernel,
        shape((rows, model), bf16),
        core,
        mine,
        from_partner(mine),
        out_gain,
        scalars=1,
    )
    return (mix_out, exp_out)


def solution(mesh):
    torus = Mesh(mesh.devices.reshape(8, 4, 8, 2), ("ep_0", "ep_1", "tp_0", "tp_1"))
    in_specs = (
        P(EP, None),
        P(),
        P(TP, None),
        P(TP, None),
        P(TP, None),
        P(TP, None),
        P(TP, None),
        P(),
        P(EP, TP),
        P(TP),
        P(EP, None),
        P(EP, None),
        P(EP, None, TP),
        P(EP, None, TP),
        P(EP, TP, None),
    )
    out_specs = (P(EP, None), P(EP, TP))

    def step(*args):
        return on_device(*args)

    step = jax.shard_map(
        step, mesh=torus, in_specs=in_specs, out_specs=out_specs, check_vma=False
    )
    return step
```

```python
import math

import jax
import jax.numpy as jnp
from jax import lax
from jax.experimental import pallas as pl
from jax.experimental.pallas import tpu as pltpu
from jax.sharding import Mesh
from jax.sharding import PartitionSpec as P

EP = ("ep_0", "ep_1")
TP = ("tp_0", "tp_1")

EPSILON = 1e-06
CLAMP_LIMIT = 7.0
SILU_SHARPNESS = 1.702
LOG2E = 1.4426950408889634
PAD = 16


def dot(a, b, dims=((1,), (0,)), precision=None):
    return lax.dot_general(
        a, b, (dims, ((), ())), precision=precision, preferred_element_type=jnp.float32
    )


def row_factor(total, width):
    return lax.rsqrt(total / width + EPSILON)


def prepare_kernel(
    routes,
    weight,
    rows,
    mix_rows,
    gain,
    w_query,
    w_key,
    w_value,
    queries,
    payload,
    table,
    every,
):
    top, tokens = routes.shape
    slots = table.shape[0]
    across, _, _ = payload.shape
    positions = mix_rows.shape[0]
    along = slots // (across * PAD)
    capacity = PAD
    slot = lax.broadcasted_iota(jnp.int32, (slots, tokens), 0)
    expert_of = slot // capacity
    place_of = slot - expert_of * capacity
    named = jnp.zeros((slots, tokens), jnp.float32)
    scale = jnp.zeros((slots, tokens), jnp.float32)
    for k in range(top):
        here = routes[k : k + 1, :] == expert_of
        named = jnp.where(here, 1.0, named)
        scale = jnp.where(here, weight[k : k + 1, :], scale)
    earlier = lax.broadcasted_iota(jnp.int32, (tokens, tokens), 0) < lax.broadcasted_iota(
        jnp.int32, (tokens, tokens), 1
    )
    earlier = jnp.where(earlier, 1.0, 0.0).astype(jnp.bfloat16)
    place = dot(named.astype(jnp.bfloat16), earlier)
    mine = (named > 0.0) & (place == place_of.astype(jnp.float32))
    table[...] = jnp.where(mine, scale, 0.0)
    chosen = jnp.where(mine, 1.0, 0.0).astype(jnp.bfloat16)
    outgoing = dot(chosen, rows[...]).astype(payload.dtype)
    for x in range(across):
        for z in range(along):
            at = (z * across + x) * capacity
            to = positions + z * capacity
            payload[x, to : to + capacity, :] = outgoing[at : at + capacity]

    numbers = mix_rows[...].astype(jnp.float32)
    factor = row_factor(jnp.sum(numbers * numbers, axis=1, keepdims=True), numbers.shape[1])
    normed = (numbers * factor * gain[...][None].astype(jnp.float32)).astype(jnp.bfloat16)
    half = positions // 2
    head = w_query.shape[0]
    every[:head, :] = w_query[...]
    every[head : 2 * head, :] = w_key[...]
    every[2 * head :, :] = w_value[...]
    both = dot(normed, every[...], ((1,), (1,))).astype(jnp.bfloat16)
    asked = both[:, :head]
    queries[...] = jnp.concatenate([asked[:half], asked[half:]], axis=1)
    pairs = both[:, head:]
    for x in range(across):
        payload[x, :positions, :] = pairs


def halves_kernel(core_ref, w_out, keep, give):
    core = core_ref[0]
    width = w_out.shape[1] // (2 * (keep.shape[1] // 128))
    for k in range(keep.shape[1] // width):
        for out, which in ((keep, core), (give, 1 - core)):
            at = pl.ds(pl.multiple_of((2 * k + which) * width, width), width)
            out[:, k * width : (k + 1) * width] = w_out[:, at]


def turn_kernel(table, turned):
    scale = table[...]
    turn = identity(scale.shape[0]).astype(jnp.bfloat16)
    for k in range(turned.shape[0]):
        piece = scale.astype(jnp.bfloat16)
        scale = scale - piece.astype(jnp.float32)
        turned[k] = dot(piece, turn, ((0,), (0,))).astype(jnp.bfloat16)


def relay_kernel(payload, queries, out):
    across = payload.shape[0]
    along = out.shape[0]
    half = queries.shape[0]
    positions = 2 * half
    own = queries[...]
    for z in range(along):
        at = slice(positions + z * PAD, positions + (z + 1) * PAD)
        for x in range(across):
            out[z, x * PAD : (x + 1) * PAD, :] = payload[x, at, :]
        out[z, across * PAD :, :] = own


def identity(size):
    row = lax.broadcasted_iota(jnp.int32, (size, size), 0)
    return jnp.where(row == lax.broadcasted_iota(jnp.int32, (size, size), 1), 1.0, 0.0)


def attend_kernel(z_ref, x_ref, payload, asked, offsets, out):
    z, x = z_ref[0], x_ref[0]
    across = payload.shape[0]
    along = asked.shape[0]
    half = asked.shape[1] - across * PAD
    rows = 2 * half
    head = asked.shape[2] // 2
    visible = lax.broadcasted_iota(jnp.int32, (rows, rows), 1) < lax.broadcasted_iota(
        jnp.int32, (rows, rows), 0
    )
    after = jnp.where(visible, -1.0, 0.0).astype(jnp.bfloat16)
    turn = identity(rows).astype(jnp.bfloat16)

    def front(q, j, diagonal):
        pair = payload[j, :rows, :]
        at = pl.multiple_of((z * across + j) * rows, rows)
        s = dot(q, pair[:, :head], ((1,), (1,)))
        s = s * (LOG2E / math.sqrt(head)) + offsets[:, pl.ds(at, rows)] * LOG2E
        soft = jnp.log2(1.0 + jnp.exp2(-jnp.abs(s)))
        take = jnp.minimum(s, 0.0) - soft
        cost = jnp.maximum(s, 0.0) + soft
        if diagonal:
            cost = jnp.where(visible, cost, 0.0)
        inside = dot(cost.astype(jnp.bfloat16), after)
        return take + inside, inside[:, :1] - cost[:, :1], pair[:, head:]

    def back(ahead, state, diagonal):
        later, acc = state
        exponent, total, values = ahead
        w = jnp.exp2(exponent + later)
        if diagonal:
            w = jnp.where(visible, w, 0.0)
        return later + total, acc + dot(w.astype(jnp.bfloat16), values)

    def asked_by(block):
        both = asked[block, across * PAD :, :]
        return jnp.concatenate([both[:, :head], both[:, head:]], axis=0)

    def send(block, state):
        later, acc = state
        acc = acc.astype(out.dtype)
        out[block, :half, :] = jnp.concatenate([acc[:half], acc[half:]], axis=1)
        high = later.astype(jnp.bfloat16)
        low = (later - high.astype(jnp.float32)).astype(jnp.bfloat16)
        wide = (rows, PAD // 2)
        parts = [jnp.broadcast_to(high, wide), jnp.broadcast_to(low, wide)]
        parts = dot(jnp.concatenate(parts, axis=1), turn, ((0,), (0,))).astype(out.dtype)
        out[block, half : half + PAD, :] = parts[:, :half]
        out[block, half + PAD :, :] = parts[:, half:]

    start = (jnp.zeros((rows, 1), jnp.float32), jnp.zeros((rows, head), jnp.float32))

    def nothing(block, carry):
        out[block] = jnp.zeros(out.shape[1:], out.dtype)
        return carry

    def everything(blocks, carry):
        asked_now = [asked_by(block) for block in blocks]
        ahead = [[front(q, across - 1 - i, False) for i in range(across)] for q in asked_now]
        for block, terms in zip(blocks, ahead):
            state = start
            for one in terms:
                state = back(one, state, False)
            send(block, state)
        return carry

    lax.fori_loop(0, z, nothing, 0)
    q = asked_by(z)
    state = back(front(q, x, True), start, True)
    state = lax.fori_loop(0, x, lambda i, c: back(front(q, x - 1 - i, False), c, False), state)
    send(z, state)
    rest = along - 1 - z
    lax.fori_loop(0, rest % 2, lambda i, c: everything([along - 1], c), 0)
    lax.fori_loop(
        0, rest // 2, lambda i, c: everything([z + 1 + 2 * i, z + 2 + 2 * i], c), 0
    )


def gather_kernel(partial, out):
    along, _, width = partial.shape
    half, head = width, width // 2
    rows = 2 * half
    turn = identity(rows).astype(jnp.bfloat16)
    later = jnp.zeros((rows, 1), jnp.float32)
    total = jnp.zeros((rows, head), jnp.float32)
    for g in range(along - 1, -1, -1):
        both = partial[g, :half, :].astype(jnp.float32)
        both = jnp.concatenate([both[:, :head], both[:, head:]], axis=0)
        total = total + jnp.exp2(later) * both
        parts = [partial[g, half : half + PAD, :], partial[g, half + PAD :, :]]
        parts = dot(turn, jnp.concatenate(parts, axis=1), ((1,), (1,)))
        later = later + (parts[:, :1] + parts[:, PAD // 2 : PAD // 2 + 1])
    total = total.astype(out.dtype)
    out[...] = jnp.concatenate([total[:half], total[half:]], axis=1)


def product_kernel(mine, theirs, keep, given, out):
    half, width = mine.shape
    head = width // 2
    top = jnp.concatenate([mine[:, :head], theirs[:, :head]], axis=1)
    low = jnp.concatenate([mine[:, head:], theirs[:, head:]], axis=1)
    side = jnp.concatenate([keep[...], given[...]], axis=0)
    top = dot(top, side).astype(out.dtype)
    low = dot(low, side).astype(out.dtype)
    size = out.shape[2]
    for k in range(out.shape[0]):
        out[k, :half, :] = top[:, k * size : (k + 1) * size]
        out[k, half:, :] = low[:, k * size : (k + 1) * size]


def total_kernel(parts, out):
    total = parts[0].astype(jnp.float32)
    for k in range(1, parts.shape[0]):
        total = total + parts[k].astype(jnp.float32)
    out[...] = total.astype(out.dtype)


def pair_kernel(mine, theirs, out):
    for k in range(out.shape[0]):
        total = mine[k].astype(jnp.float32) + theirs[k].astype(jnp.float32)
        out[k] = total.astype(out.dtype)


def mix_norm_kernel(columns, gain, out):
    parts, rows, width = columns.shape
    total = jnp.zeros((rows, 1), jnp.float32)
    for k in range(parts):
        numbers = columns[k].astype(jnp.float32)
        total = total + jnp.sum(numbers * numbers, axis=1, keepdims=True)
    factor = row_factor(total, parts * width)
    scale = gain[...].astype(jnp.float32)[None]
    for k in range(parts):
        at = slice(k * width, (k + 1) * width)
        numbers = columns[k].astype(jnp.float32) * factor * scale[:, at]
        out[:, at] = numbers.astype(out.dtype)


def expert_kernel(core_ref, arrived, w_gate, w_up, w_down, keep, give, scaled, both):
    core = core_ref[0]
    parts, padded, width = arrived.shape
    rows = padded - PAD
    hidden = w_gate.shape[2]
    both[:, :hidden] = w_gate[0]
    both[:, hidden:] = w_up[0]
    total = jnp.zeros((rows, width), jnp.float32)
    for k in range(parts):
        numbers = arrived[k, :rows, :].astype(jnp.float32)
        total = total + numbers * numbers
        gain = arrived[k, rows : rows + 1, :].astype(jnp.float32)
        scaled[:, k * width : (k + 1) * width] = (numbers * gain).astype(jnp.bfloat16)
    factor = row_factor(jnp.sum(total, axis=1, keepdims=True), parts * width)
    pre = dot(scaled[...], both[...]) * factor
    gate = jnp.minimum(pre[:, :hidden], CLAMP_LIMIT)
    up = jnp.clip(pre[:, hidden:], -CLAMP_LIMIT, CLAMP_LIMIT)
    units = (up + 1.0) * (gate * jax.nn.sigmoid(SILU_SHARPNESS * gate))
    units = units.astype(keep.dtype)
    for k in range(keep.shape[0]):
        for out, which in ((keep, core), (give, 1 - core)):
            at = pl.ds(pl.multiple_of((2 * k + which) * width, width), width)
            out[k] = dot(units, w_down[0, :, at]).astype(out.dtype)


def call(body, outs, *args, scalars=0, **kwargs):
    spaces = [pltpu.SMEM] * scalars + [pltpu.VMEM] * (len(args) - scalars)
    specs = [pl.BlockSpec(memory_space=space) for space in spaces]
    return pl.pallas_call(body, out_shape=outs, in_specs=specs, **kwargs)(*args)


def exchanged(value, axis):
    return lax.all_to_all(value, axis, 0, 0, tiled=True)


def from_partner(value):
    return lax.ppermute(value, "tp_1", [(0, 1), (1, 0)])


def on_device(
    mix_rows,
    mix_gain,
    w_query,
    w_key,
    w_value,
    key_offset,
    w_out,
    out_gain,
    exp_rows,
    exp_gain,
    routes,
    route_weight,
    w_gate,
    w_up,
    w_down,
):
    bf16 = jnp.bfloat16
    shape = jax.ShapeDtypeStruct
    ep_count = lax.axis_size(EP)
    tp_count = lax.axis_size(TP)
    tokens, top = routes.shape
    part = exp_rows.shape[1]
    experts = ep_count * w_gate.shape[0]
    capacity = 4 * tokens * top // (3 * experts)
    slots = experts * capacity
    rows = mix_rows.shape[0]
    head = w_query.shape[0]
    model = mix_rows.shape[1]
    core = lax.axis_index("tp_1").astype(jnp.int32)[None]

    across = lax.axis_size("ep_1")
    along = lax.axis_size("ep_0")
    half = rows // 2
    queries, payload, table = call(
        prepare_kernel,
        (
            shape((half, 2 * head), bf16),
            shape((across, rows + along * capacity, part), bf16),
            shape((slots, tokens), jnp.float32),
        ),
        routes.T,
        route_weight.T,
        exp_rows,
        mix_rows,
        mix_gain,
        w_query,
        w_key,
        w_value,
        scratch_shapes=[pltpu.VMEM((3 * head, model), bf16)],
    )
    payload = exchanged(payload, "ep_1")
    asked = call(
        relay_kernel,
        shape((along, across * capacity + half, part), bf16),
        payload,
        queries,
    )
    asked = exchanged(asked, "ep_0")
    arrived = asked[:, : across * capacity].reshape(slots, part)
    gain_rows = jnp.broadcast_to(exp_gain[None], (PAD, part))
    every_row = jnp.concatenate([arrived, gain_rows], axis=0)
    every_row = lax.all_gather(every_row, TP, axis=0)

    groups = tp_count // 2
    size = model // tp_count
    keep_out, give_out = call(
        halves_kernel,
        (shape((head, groups * size), bf16), shape((head, groups * size), bf16)),
        core,
        w_out,
        scalars=1,
    )
    given_out = from_partner(give_out)
    turned = call(turn_kernel, shape((2, tokens, slots), bf16), table)

    partial = call(
        attend_kernel,
        shape((along, half + 2 * PAD, 2 * head), bf16),
        lax.axis_index("ep_0").astype(jnp.int32)[None],
        lax.axis_index("ep_1").astype(jnp.int32)[None],
        payload,
        asked,
        key_offset,
        scalars=2,
    )
    partial = exchanged(partial, "ep_0")
    attended = call(gather_kernel, shape((half, 2 * head), bf16), partial)

    products = call(
        product_kernel,
        shape((groups, rows, size), bf16),
        attended,
        from_partner(attended),
        keep_out,
        given_out,
    )
    products = exchanged(products, "tp_0")
    own_columns = call(total_kernel, shape((rows, size), bf16), products)
    every_column = lax.all_gather(own_columns, TP, axis=0)
    mix_out = call(mix_norm_kernel, shape((rows, model), bf16), every_column, out_gain)

    units = w_gate.shape[2]
    keep, give = call(
        expert_kernel,
        (shape((groups, slots, size), bf16), shape((groups, slots, size), bf16)),
        core,
        every_row,
        w_gate,
        w_up,
        w_down,
        scalars=1,
        scratch_shapes=[
            pltpu.VMEM((slots, model), bf16),
            pltpu.VMEM((model, 2 * units), bf16),
        ],
    )
    sums = call(
        pair_kernel, shape((groups, slots, size), bf16), keep, from_partner(give)
    )
    sums = exchanged(sums, "tp_0")
    expert_out = call(total_kernel, shape((slots, size), bf16), sums)
    returned = exchanged(expert_out, EP).reshape(slots, part)
    combined = dot(turned.reshape(2 * tokens, slots), returned).reshape(2, tokens, part)
    exp_out = (combined[0] + combined[1]).astype(bf16)
    return (mix_out, exp_out)


def solution(mesh):
    torus = Mesh(mesh.devices.reshape(8, 4, 8, 2), ("ep_0", "ep_1", "tp_0", "tp_1"))
    in_specs = (
        P(EP, None),
        P(),
        P(TP, None),
        P(TP, None),
        P(TP, None),
        P(TP, None),
        P(TP, None),
        P(),
        P(EP, TP),
        P(TP),
        P(EP, None),
        P(EP, None),
        P(EP, None, TP),
        P(EP, None, TP),
        P(EP, TP, None),
    )
    out_specs = (P(EP, None), P(EP, TP))

    def step(*args):
        return on_device(*args)

    step = jax.shard_map(
        step, mesh=torus, in_specs=in_specs, out_specs=out_specs, check_vma=False
    )
    return step
```

```python
import math

import jax
import jax.numpy as jnp
from jax import lax
from jax.experimental import pallas as pl
from jax.experimental.pallas import tpu as pltpu
from jax.sharding import Mesh
from jax.sharding import PartitionSpec as P

EP = ("ep_0", "ep_1")
TP = ("tp_0", "tp_1")

EPSILON = 1e-06
CLAMP_LIMIT = 7.0
SILU_SHARPNESS = 1.702
LOG2E = 1.4426950408889634
PAD = 16


def dot(a, b, dims=((1,), (0,)), precision=None):
    return lax.dot_general(
        a, b, (dims, ((), ())), precision=precision, preferred_element_type=jnp.float32
    )


def row_factor(total, width):
    return lax.rsqrt(total / width + EPSILON)


def prepare_kernel(
    routes,
    weight,
    rows,
    mix_rows,
    gain,
    w_query,
    w_key,
    w_value,
    queries,
    payload,
    table,
    every,
):
    top, tokens = routes.shape
    slots = table.shape[0]
    across, _, _ = payload.shape
    positions = mix_rows.shape[0]
    along = slots // (across * PAD)
    capacity = PAD
    slot = lax.broadcasted_iota(jnp.int32, (slots, tokens), 0)
    expert_of = slot // capacity
    place_of = slot - expert_of * capacity
    named = jnp.zeros((slots, tokens), jnp.float32)
    scale = jnp.zeros((slots, tokens), jnp.float32)
    for k in range(top):
        here = routes[k : k + 1, :] == expert_of
        named = jnp.where(here, 1.0, named)
        scale = jnp.where(here, weight[k : k + 1, :], scale)
    earlier = lax.broadcasted_iota(jnp.int32, (tokens, tokens), 0) < lax.broadcasted_iota(
        jnp.int32, (tokens, tokens), 1
    )
    earlier = jnp.where(earlier, 1.0, 0.0).astype(jnp.bfloat16)
    place = dot(named.astype(jnp.bfloat16), earlier)
    mine = (named > 0.0) & (place == place_of.astype(jnp.float32))
    table[...] = jnp.where(mine, scale, 0.0)
    chosen = jnp.where(mine, 1.0, 0.0).astype(jnp.bfloat16)
    outgoing = dot(chosen, rows[...]).astype(payload.dtype)
    for x in range(across):
        for z in range(along):
            at = (z * across + x) * capacity
            to = positions + z * capacity
            payload[x, to : to + capacity, :] = outgoing[at : at + capacity]

    numbers = mix_rows[...].astype(jnp.float32)
    factor = row_factor(jnp.sum(numbers * numbers, axis=1, keepdims=True), numbers.shape[1])
    normed = (numbers * factor * gain[...][None].astype(jnp.float32)).astype(jnp.bfloat16)
    half = positions // 2
    head = w_query.shape[0]
    every[:head, :] = w_query[...]
    every[head : 2 * head, :] = w_key[...]
    every[2 * head :, :] = w_value[...]
    both = dot(normed, every[...], ((1,), (1,))).astype(jnp.bfloat16)
    asked = both[:, :head]
    queries[...] = jnp.concatenate([asked[:half], asked[half:]], axis=1)
    pairs = both[:, head:]
    for x in range(across):
        payload[x, :positions, :] = pairs


def halves_kernel(core_ref, w_out, w_down, keep, give, keep_down, give_down):
    core = core_ref[0]
    width = 128
    for k in range(keep.shape[1] // width):
        to = slice(k * width, (k + 1) * width)
        for out, down, which in ((keep, keep_down, core), (give, give_down, 1 - core)):
            at = pl.ds(pl.multiple_of((2 * k + which) * width, width), width)
            out[:, to] = w_out[:, at]
            down[:, to] = w_down[0, :, at]


def turn_kernel(table, turned):
    scale = table[...]
    turn = identity(scale.shape[0]).astype(jnp.bfloat16)
    for k in range(turned.shape[0]):
        piece = scale.astype(jnp.bfloat16)
        scale = scale - piece.astype(jnp.float32)
        turned[k] = dot(piece, turn, ((0,), (0,))).astype(jnp.bfloat16)


def relay_kernel(payload, queries, out):
    across = payload.shape[0]
    along = out.shape[0]
    half = queries.shape[0]
    positions = 2 * half
    own = queries[...]
    for z in range(along):
        at = slice(positions + z * PAD, positions + (z + 1) * PAD)
        for x in range(across):
            out[z, x * PAD : (x + 1) * PAD, :] = payload[x, at, :]
        out[z, across * PAD :, :] = own


def identity(size):
    row = lax.broadcasted_iota(jnp.int32, (size, size), 0)
    return jnp.where(row == lax.broadcasted_iota(jnp.int32, (size, size), 1), 1.0, 0.0)


def attend_kernel(z_ref, x_ref, payload, asked, offsets, out):
    z, x = z_ref[0], x_ref[0]
    across = payload.shape[0]
    along = asked.shape[0]
    half = asked.shape[1] - across * PAD
    rows = 2 * half
    head = asked.shape[2] // 2
    visible = lax.broadcasted_iota(jnp.int32, (rows, rows), 1) < lax.broadcasted_iota(
        jnp.int32, (rows, rows), 0
    )
    after = jnp.where(visible, -1.0, 0.0).astype(jnp.bfloat16)
    turn = identity(rows).astype(jnp.bfloat16)

    def front(q, j, diagonal):
        pair = payload[j, :rows, :]
        at = pl.multiple_of((z * across + j) * rows, rows)
        s = dot(q, pair[:, :head], ((1,), (1,)))
        s = s * (LOG2E / math.sqrt(head)) + offsets[:, pl.ds(at, rows)] * LOG2E
        soft = jnp.log2(1.0 + jnp.exp2(-jnp.abs(s)))
        take = jnp.minimum(s, 0.0) - soft
        cost = jnp.maximum(s, 0.0) + soft
        if diagonal:
            cost = jnp.where(visible, cost, 0.0)
        inside = dot(cost.astype(jnp.bfloat16), after)
        return take + inside, inside[:, :1] - cost[:, :1], pair[:, head:]

    def back(ahead, state, diagonal):
        later, acc = state
        exponent, total, values = ahead
        w = jnp.exp2(exponent + later)
        if diagonal:
            w = jnp.where(visible, w, 0.0)
        return later + total, acc + dot(w.astype(jnp.bfloat16), values)

    def asked_by(block):
        both = asked[block, across * PAD :, :]
        return jnp.concatenate([both[:, :head], both[:, head:]], axis=0)

    def send(block, state):
        later, acc = state
        acc = acc.astype(out.dtype)
        out[block, :half, :] = jnp.concatenate([acc[:half], acc[half:]], axis=1)
        high = later.astype(jnp.bfloat16)
        low = (later - high.astype(jnp.float32)).astype(jnp.bfloat16)
        wide = (rows, PAD // 2)
        parts = [jnp.broadcast_to(high, wide), jnp.broadcast_to(low, wide)]
        parts = dot(jnp.concatenate(parts, axis=1), turn, ((0,), (0,))).astype(out.dtype)
        out[block, half : half + PAD, :] = parts[:, :half]
        out[block, half + PAD :, :] = parts[:, half:]

    start = (jnp.zeros((rows, 1), jnp.float32), jnp.zeros((rows, head), jnp.float32))

    def nothing(block, carry):
        out[block] = jnp.zeros(out.shape[1:], out.dtype)
        return carry

    def everything(blocks, carry):
        asked_now = [asked_by(block) for block in blocks]
        ahead = [[front(q, across - 1 - i, False) for i in range(across)] for q in asked_now]
        for block, terms in zip(blocks, ahead):
            state = start
            for one in terms:
                state = back(one, state, False)
            send(block, state)
        return carry

    lax.fori_loop(0, z, nothing, 0)
    q = asked_by(z)
    state = back(front(q, x, True), start, True)
    state = lax.fori_loop(0, x, lambda i, c: back(front(q, x - 1 - i, False), c, False), state)
    send(z, state)
    rest = along - 1 - z
    lax.fori_loop(0, rest % 2, lambda i, c: everything([along - 1], c), 0)
    lax.fori_loop(
        0, rest // 2, lambda i, c: everything([z + 1 + 2 * i, z + 2 + 2 * i], c), 0
    )


def gather_kernel(partial, out):
    along, _, width = partial.shape
    half, head = width, width // 2
    rows = 2 * half
    turn = identity(rows).astype(jnp.bfloat16)
    later = jnp.zeros((rows, 1), jnp.float32)
    total = jnp.zeros((rows, head), jnp.float32)
    for g in range(along - 1, -1, -1):
        both = partial[g, :half, :].astype(jnp.float32)
        both = jnp.concatenate([both[:, :head], both[:, head:]], axis=0)
        total = total + jnp.exp2(later) * both
        parts = [partial[g, half : half + PAD, :], partial[g, half + PAD :, :]]
        parts = dot(turn, jnp.concatenate(parts, axis=1), ((1,), (1,)))
        later = later + (parts[:, :1] + parts[:, PAD // 2 : PAD // 2 + 1])
    total = total.astype(out.dtype)
    out[...] = jnp.concatenate([total[:half], total[half:]], axis=1)


def product_kernel(mine, theirs, keep, given, out):
    half, width = mine.shape
    head = width // 2
    top = jnp.concatenate([mine[:, :head], theirs[:, :head]], axis=1)
    low = jnp.concatenate([mine[:, head:], theirs[:, head:]], axis=1)
    side = jnp.concatenate([keep[...], given[...]], axis=0)
    top = dot(top, side).astype(out.dtype)
    low = dot(low, side).astype(out.dtype)
    size = out.shape[2]
    for k in range(out.shape[0]):
        out[k, :half, :] = top[:, k * size : (k + 1) * size]
        out[k, half:, :] = low[:, k * size : (k + 1) * size]


def mix_norm_kernel(columns, gain, out):
    parts, rows, width = columns.shape
    total = jnp.zeros((rows, 1), jnp.float32)
    for k in range(parts):
        numbers = columns[k].astype(jnp.float32)
        total = total + jnp.sum(numbers * numbers, axis=1, keepdims=True)
    factor = row_factor(total, parts * width)
    scale = gain[...].astype(jnp.float32)[None]
    for k in range(parts):
        at = slice(k * width, (k + 1) * width)
        numbers = columns[k].astype(jnp.float32) * factor * scale[:, at]
        out[:, at] = numbers.astype(out.dtype)


def expert_kernel(
    arrived, w_gate, w_up, keep_down, give_down, keep, give, scaled, both
):
    parts, padded, width = arrived.shape
    rows = padded - PAD
    hidden = w_gate.shape[2]
    both[:, :hidden] = w_gate[0]
    both[:, hidden:] = w_up[0]
    total = jnp.zeros((rows, width), jnp.float32)
    for k in range(parts):
        numbers = arrived[k, :rows, :].astype(jnp.float32)
        total = total + numbers * numbers
        gain = arrived[k, rows : rows + 1, :].astype(jnp.float32)
        scaled[:, k * width : (k + 1) * width] = (numbers * gain).astype(jnp.bfloat16)
    factor = row_factor(jnp.sum(total, axis=1, keepdims=True), parts * width)
    pre = dot(scaled[...], both[...]) * factor
    gate = jnp.minimum(pre[:, :hidden], CLAMP_LIMIT)
    up = jnp.clip(pre[:, hidden:], -CLAMP_LIMIT, CLAMP_LIMIT)
    units = (up + 1.0) * (gate * jax.nn.sigmoid(SILU_SHARPNESS * gate))
    units = units.astype(keep.dtype)
    for out, down in ((give, give_down), (keep, keep_down)):
        product = dot(units, down[...]).astype(out.dtype)
        for k in range(out.shape[0]):
            out[k] = product[:, k * width : (k + 1) * width]


def call(body, outs, *args, scalars=0, **kwargs):
    spaces = [pltpu.SMEM] * scalars + [pltpu.VMEM] * (len(args) - scalars)
    specs = [pl.BlockSpec(memory_space=space) for space in spaces]
    return pl.pallas_call(body, out_shape=outs, in_specs=specs, **kwargs)(*args)


def total(parts):
    return jnp.sum(parts.astype(jnp.float32), axis=0).astype(parts.dtype)


def exchanged(value, axis):
    return lax.all_to_all(value, axis, 0, 0, tiled=True)


def from_partner(value):
    return lax.ppermute(value, "tp_1", [(0, 1), (1, 0)])


def on_device(
    mix_rows,
    mix_gain,
    w_query,
    w_key,
    w_value,
    key_offset,
    w_out,
    out_gain,
    exp_rows,
    exp_gain,
    routes,
    route_weight,
    w_gate,
    w_up,
    w_down,
):
    bf16 = jnp.bfloat16
    shape = jax.ShapeDtypeStruct
    ep_count = lax.axis_size(EP)
    tp_count = lax.axis_size(TP)
    tokens, top = routes.shape
    part = exp_rows.shape[1]
    experts = ep_count * w_gate.shape[0]
    capacity = 4 * tokens * top // (3 * experts)
    slots = experts * capacity
    rows = mix_rows.shape[0]
    head = w_query.shape[0]
    model = mix_rows.shape[1]
    core = lax.axis_index("tp_1").astype(jnp.int32)[None]

    across = lax.axis_size("ep_1")
    along = lax.axis_size("ep_0")
    half = rows // 2
    queries, payload, table = call(
        prepare_kernel,
        (
            shape((half, 2 * head), bf16),
            shape((across, rows + along * capacity, part), bf16),
            shape((slots, tokens), jnp.float32),
        ),
        routes.T,
        route_weight.T,
        exp_rows,
        mix_rows,
        mix_gain,
        w_query,
        w_key,
        w_value,
        scratch_shapes=[pltpu.VMEM((3 * head, model), bf16)],
    )
    payload = exchanged(payload, "ep_1")
    asked = call(
        relay_kernel,
        shape((along, across * capacity + half, part), bf16),
        payload,
        queries,
    )
    asked = exchanged(asked, "ep_0")
    arrived = asked[:, : across * capacity].reshape(slots, part)
    gain_rows = jnp.broadcast_to(exp_gain[None], (PAD, part))
    every_row = jnp.concatenate([arrived, gain_rows], axis=0)
    every_row = lax.all_gather(every_row, TP, axis=0)

    groups = tp_count // 2
    size = model // tp_count
    part_out = shape((head, groups * size), bf16)
    part_down = shape((w_down.shape[1], groups * size), bf16)
    keep_out, give_out, keep_down, give_down = call(
        halves_kernel,
        (part_out, part_out, part_down, part_down),
        core,
        w_out,
        w_down,
        scalars=1,
    )
    given_out = from_partner(give_out)
    turned = call(turn_kernel, shape((2, tokens, slots), bf16), table)

    partial = call(
        attend_kernel,
        shape((along, half + 2 * PAD, 2 * head), bf16),
        lax.axis_index("ep_0").astype(jnp.int32)[None],
        lax.axis_index("ep_1").astype(jnp.int32)[None],
        payload,
        asked,
        key_offset,
        scalars=2,
    )
    partial = exchanged(partial, "ep_0")
    attended = call(gather_kernel, shape((half, 2 * head), bf16), partial)

    products = call(
        product_kernel,
        shape((groups, rows, size), bf16),
        attended,
        from_partner(attended),
        keep_out,
        given_out,
    )
    products = exchanged(products, "tp_0")
    own_columns = total(products)
    units = w_gate.shape[2]
    keep, give = call(
        expert_kernel,
        (shape((groups, slots, size), bf16), shape((groups, slots, size), bf16)),
        every_row,
        w_gate,
        w_up,
        keep_down,
        give_down,
        scratch_shapes=[
            pltpu.VMEM((slots, model), bf16),
            pltpu.VMEM((model, 2 * units), bf16),
        ],
    )
    sums = keep.astype(jnp.float32) + from_partner(give).astype(jnp.float32)
    sums = sums.astype(bf16)
    sums, own_columns = lax.optimization_barrier((sums, own_columns))
    every_column = lax.all_gather(own_columns, TP, axis=0)
    mix_out = call(mix_norm_kernel, shape((rows, model), bf16), every_column, out_gain)
    sums = exchanged(sums, "tp_0")
    expert_out = total(sums)
    returned = exchanged(expert_out, EP).reshape(slots, part)
    combined = dot(turned.reshape(2 * tokens, slots), returned).reshape(2, tokens, part)
    exp_out = (combined[0] + combined[1]).astype(bf16)
    return (mix_out, exp_out)


def solution(mesh):
    torus = Mesh(mesh.devices.reshape(8, 4, 8, 2), ("ep_0", "ep_1", "tp_0", "tp_1"))
    in_specs = (
        P(EP, None),
        P(),
        P(TP, None),
        P(TP, None),
        P(TP, None),
        P(TP, None),
        P(TP, None),
        P(),
        P(EP, TP),
        P(TP),
        P(EP, None),
        P(EP, None),
        P(EP, None, TP),
        P(EP, None, TP),
        P(EP, TP, None),
    )
    out_specs = (P(EP, None), P(EP, TP))

    def step(*args):
        return on_device(*args)

    step = jax.shard_map(
        step, mesh=torus, in_specs=in_specs, out_specs=out_specs, check_vma=False
    )
    return step
```
